256 devices in a mesh: kv: 32 (over z, x), tp: 8 (over y, core).
Axes of the slice: x: 4, y: 4, z: 8, core: 2. Of those that a mesh axis runs over, the one named last changes fastest.
Arguments:
- tokens: bfloat16 [4096, 2048], P('kv', 'tp'), may hold values from -6 to 6
- states: float32 [4096, 16, 64, 64], P('kv', 'tp'), may hold values from -6 to 6
- mix_gain: bfloat16 [2048], replicated, may hold values from 0.099609375 to 1.8984375
- w_query: bfloat16 [2048, 1024], P(None, 'tp'), may hold values from -0.125 to 0.125
- w_key: bfloat16 [2048, 1024], P(None, 'tp'), may hold values from -0.125 to 0.125
- w_value: bfloat16 [2048, 1024], P(None, 'tp'), may hold values from -0.125 to 0.125
- w_gate: bfloat16 [2048, 1024], P(None, 'tp'), may hold values from -0.125 to 0.125
- head_gain: bfloat16 [1024], P('tp'), may hold values from 0.099609375 to 1.8984375
- w_output: bfloat16 [1024, 2048], P('tp'), may hold values from -0.1875 to 0.1875
- channel_gain: bfloat16 [2048], replicated, may hold values from 0.099609375 to 1.8984375
- w_up: bfloat16 [2048, 8192], P(None, 'kv'), may hold values from -0.125 to 0.125
- w_down: bfloat16 [8192, 2048], P('kv'), may hold values from -0.0625 to 0.0625
Outputs:
- layer_out: bfloat16 [4096, 2048], P('kv', 'tp')
- new_states: float32 [4096, 16, 64, 64], P('kv', 'tp')
The draws below stay inside these ranges and needn't reach their ends.
All inputs are finite; a program needn't handle non-finite values.
Results may differ from the reference program's by a relative error of at most 0.019.
Values may be sent and summed in bfloat16 or wider, within the bound.
No kernel may reach another device: no remote copies, remote signals or barrier semaphores. Data moves between devices by JAX's collectives and lax.ppermute only.
A program may use at most 64 MiB of HBM per device.

```python
import jax
import jax.numpy as jnp
from jax import lax

D = 2048
HEADS = 16
HEAD = 64
FF = 8192
POS = 16384
BATCH = 4096
N_TP = 8


def draw_tokens(key, part):
    first_key = jax.random.fold_in(jax.random.fold_in(key, 11), 0)
    column = jnp.arange(D, dtype=jnp.float32) / D
    profile = 0.5 * jnp.exp(jnp.log(3.0) * column)
    drawn = jax.random.normal(first_key, (BATCH, D), jnp.float32) * profile
    return jnp.clip(drawn, -6.0, 6.0).astype(jnp.bfloat16)


def shard_levels(rng, extent, shards, smallest, high):
    gain = 1.0
    for dim, parts in shards:
        steps = jax.random.uniform(jax.random.fold_in(jax.random.fold_in(rng, 6), dim), (parts,), jnp.float32, smallest / len(shards), high / len(shards))
        gain = gain * jnp.repeat(jnp.exp(steps), extent[dim] // parts).reshape((-1,) + (1,) * (len(extent) - 1 - dim))
    return gain


def scatter_about(rng, extent, scale, bound, shards=(), kind=jnp.bfloat16):
    array = jax.random.normal(rng, extent, jnp.float32) * scale
    if len(shards) > 0:
        array = shard_levels(rng, extent, shards, -0.22, 0.18) * array
    return jnp.clip(array, min=-bound, max=bound).astype(kind)


def setup_inputs(seed: int = 0) -> dict:
    arg_keys = jax.random.split(jax.random.key(seed), 13)
    return {
        "tokens": draw_tokens(jax.random.fold_in(arg_keys[12], 71), 0),
        "states": scatter_about(arg_keys[1], (BATCH, HEADS, HEAD, HEAD), 1.0, 6.0, ((0, 32), (1, 8)), jnp.float32),
        "mix_gain": jnp.clip(1.0 + 0.18 * jax.random.normal(arg_keys[2], (D,), jnp.float32), 0.099609375, 1.8984375).astype(jnp.bfloat16),
        "w_query": scatter_about(arg_keys[3], (D, HEADS * HEAD), D ** -0.5, 0.125, ((1, 8),)),
        "w_key": scatter_about(arg_keys[4], (D, HEADS * HEAD), D ** -0.5, 0.125, ((1, 8),)),
        "w_value": scatter_about(arg_keys[5], (D, HEADS * HEAD), D ** -0.5, 0.125, ((1, 8),)),
        "w_gate": scatter_about(arg_keys[6], (D, HEADS * HEAD), D ** -0.5, 0.125, ((1, 8),)),
        "head_gain": jnp.clip(1.0 + 0.18 * jax.random.normal(arg_keys[7], (HEADS * HEAD,), jnp.float32), 0.099609375, 1.8984375).astype(jnp.bfloat16),
        "w_output": scatter_about(arg_keys[8], (HEADS * HEAD, D), (HEADS * HEAD) ** -0.5, 0.1875, ((0, 8),)),
        "channel_gain": jnp.clip(1.0 + 0.18 * jax.random.normal(arg_keys[9], (D,), jnp.float32), 0.099609375, 1.8984375).astype(jnp.bfloat16),
        "w_up": scatter_about(arg_keys[10], (D, FF), D ** -0.5, 0.125, ((1, 32),)),
        "w_down": scatter_about(arg_keys[11], (FF, D), FF ** -0.5, 0.0625, ((0, 32),)),
    }


EPSILON = 1e-06
ROTARY_BASE = 10000.0

def rotate(vectors):
    half_size = vectors.shape[-1] // 2
    frequency = ROTARY_BASE ** (-jnp.arange(half_size, dtype=jnp.float32) / half_size)
    angles = POS * frequency
    cosine = jnp.cos(angles)
    sines = jnp.sin(angles)
    first_half = vectors[..., :half_size]
    second = vectors[..., half_size:]
    return jnp.concatenate([first_half * cosine - second * sines, first_half * sines + second * cosine], axis=-1)

def retain(normed, states, w_query, w_key, w_value, w_gate, head_gain, head_ids):
    row_count = states.shape[0]
    head_count = states.shape[1]
    head_size = states.shape[2]

    def project(weight):
        return jnp.dot(normed, weight, preferred_element_type=jnp.float32).reshape(row_count, head_count, head_size)
    queries = rotate(project(w_query)) * head_size ** (-0.5)
    keys_now = rotate(project(w_key))
    values = project(w_value)
    gating = jnp.dot(normed, w_gate, preferred_element_type=jnp.float32)
    decays = 1.0 - jnp.exp2(-1.0 - 11.0 * head_ids / (HEADS - 1))
    new_states = decays[None, :, None, None] * states + keys_now[:, :, :, None] * values[:, :, None, :]
    output = jnp.einsum('bhk,bhkv->bhv', queries, new_states, precision=lax.Precision.HIGHEST)
    center = output - lax.optimization_barrier(jnp.mean(output, axis=-1, keepdims=True))
    spread = lax.optimization_barrier(jnp.mean(center * center, axis=-1, keepdims=True))
    scaled = center * lax.rsqrt(spread + EPSILON) * head_gain.astype(jnp.float32).reshape(head_count, head_size)
    gated_out = (scaled.reshape(row_count, head_count * head_size) * jax.nn.silu(gating)).astype(jnp.bfloat16)
    return (gated_out, new_states)

def reference(tokens, states, mix_gain, w_query, w_key, w_value, w_gate, head_gain, w_output, channel_gain, w_up, w_down):
    widened = tokens.astype(jnp.float32)
    inverse_rms = lax.rsqrt(lax.optimization_barrier(jnp.mean(widened * widened, axis=1, keepdims=True)) + EPSILON)
    normed = (widened * inverse_rms * mix_gain.astype(jnp.float32)).astype(jnp.bfloat16)
    head_ids = jnp.arange(HEADS).astype(jnp.float32)
    gated_out, new_states = retain(normed, states, w_query, w_key, w_value, w_gate, head_gain, head_ids)
    blocks = gated_out.astype(jnp.float32).reshape(BATCH, N_TP, -1)
    weights = w_output.astype(jnp.float32).reshape(N_TP, -1, D)
    partials = jnp.einsum('btc,tcd->btd', blocks, weights)
    rounded = lax.optimization_barrier(partials.astype(jnp.bfloat16))
    attended = lax.optimization_barrier(jnp.sum(rounded.astype(jnp.float32), axis=1))
    middle = (widened + attended).astype(jnp.bfloat16)
    mid_wide = middle.astype(jnp.float32)
    second_rms = lax.rsqrt(lax.optimization_barrier(jnp.mean(mid_wide * mid_wide, axis=1, keepdims=True)) + EPSILON)
    scaled = (mid_wide * channel_gain.astype(jnp.float32)).astype(jnp.bfloat16)
    hidden = jnp.dot(scaled, w_up, preferred_element_type=jnp.float32) * second_rms
    activated = jnp.square(jax.nn.relu(hidden)).astype(jnp.bfloat16)
    down_sum = jnp.dot(activated, w_down, preferred_element_type=jnp.float32)
    layer_out = (mid_wide + down_sum).astype(jnp.bfloat16)
    return (layer_out, new_states)
```

```python
import jax
import jax.numpy as jnp
from jax import lax
from jax.experimental import pallas as pl
from jax.experimental.pallas import tpu as pltpu
from jax.sharding import Mesh
from jax.sharding import PartitionSpec as P

HEADS = 16
HEAD = 64
POS = 16384
D = 2048
EPSILON = 1e-06
ROTARY_BASE = 10000.0
ROWS = 128
Z, X, Y, C = 8, 4, 4, 2
TP = Y * C
SHARE = ROWS // TP
F32 = jnp.float32
BF16 = jnp.bfloat16


def copy_all(copies):
    for copy in copies:
        copy.start()
    for copy in copies:
        copy.wait()


def pack_kernel(up, down, packed, sems):
    at = pl.multiple_of(lax.axis_index("c") * 128, 128)
    copies = [
        pltpu.make_async_copy(
            up.at[pl.ds(8 * i, 8), :, pl.ds(at, 128)],
            packed.at[pl.ds(0, 8), :, pl.ds(128 * i, 128)],
            sems.at[i],
        )
        for i in range(2)
    ]
    copies += [
        pltpu.make_async_copy(
            down.at[pl.ds(at, 128), pl.ds(256 * j, 256)], packed.at[8 + j], sems.at[2 + j]
        )
        for j in range(8)
    ]
    copy_all(copies)


def pack(w_up, w_down):
    return pl.pallas_call(
        pack_kernel,
        out_shape=jax.ShapeDtypeStruct((16, 128, 256), BF16),
        in_specs=[pl.BlockSpec(memory_space=pl.ANY)] * 2,
        out_specs=pl.BlockSpec(memory_space=pl.ANY),
        scratch_shapes=[pltpu.SemaphoreType.DMA((10,))],
        name="pack",
    )(w_up.reshape(16, 128, 256), w_down)


CHUNKS = 8
PER_HEAD = CHUNKS // 2
STEP = HEAD // PER_HEAD


def retain_kernel(
    decays, tokens, states, wq, wk, wv, wg, mix_gain, head_gain, cosine, sines,
    new_states, gated, weights, old, new, qt, kt, ret, w_sems, in_sems, out_sems,
):
    def part(ref, i):
        return ref.at[i // PER_HEAD, pl.ds((i % PER_HEAD) * STEP, STEP)]

    w_copies = [
        pltpu.make_async_copy(w, weights.at[:, pl.ds(128 * i, 128)], w_sems.at[i])
        for i, w in enumerate((wq, wk, wv, wg))
    ]
    in_copies = [
        pltpu.make_async_copy(part(states, i), part(old, i), in_sems.at[i]) for i in range(CHUNKS)
    ]
    out_copies = [
        pltpu.make_async_copy(part(new, i), part(new_states, i), out_sems.at[i])
        for i in range(CHUNKS)
    ]
    for copy in w_copies + in_copies:
        copy.start()

    squares = jnp.zeros((ROWS, 256), F32)
    for j in range(TP):
        block = tokens[j].astype(F32)
        squares += block * block
    inverse_rms = lax.rsqrt(jnp.sum(squares, axis=1, keepdims=True) / D + EPSILON)
    normed = [
        (tokens[j].astype(F32) * inverse_rms * mix_gain[:, 256 * j : 256 * j + 256].astype(F32))
        .astype(BF16)
        for j in range(TP)
    ]
    for copy in w_copies:
        copy.wait()
    projected = jnp.zeros((ROWS, 512), F32)
    for j in range(TP):
        projected += jnp.dot(
            normed[j], weights[256 * j : 256 * j + 256, :], preferred_element_type=F32
        )
    half = HEAD // 2

    def turned(flat):
        rows = []
        for h in range(2):
            a = flat[h * HEAD : h * HEAD + half]
            b = flat[h * HEAD + half : (h + 1) * HEAD]
            rows += [a * cosine[...] - b * sines[...], a * sines[...] + b * cosine[...]]
        return jnp.concatenate(rows, axis=0)

    qt[...] = turned(projected[:, 0:128].T) * HEAD**-0.5
    kt[...] = turned(projected[:, 128:256].T)
    vt = projected[:, 256:384].T
    gating = projected[:, 384:512]

    for h in range(2):
        values = vt[h * HEAD : (h + 1) * HEAD]
        decay = decays[h]
        total = jnp.zeros((HEAD, ROWS), F32)
        for i in range(h * PER_HEAD, (h + 1) * PER_HEAD):
            in_copies[i].wait()
            first = (i % PER_HEAD) * STEP

            def step(s, total):
                k = first + s
                row = h * HEAD + k
                fresh = decay * old[h, k] + kt[pl.ds(row, 1), :] * values
                new[h, k] = fresh
                return total + qt[pl.ds(row, 1), :] * fresh

            total = lax.fori_loop(0, STEP, step, total, unroll=8)
            out_copies[i].start()
        center = total - jnp.mean(total, axis=0, keepdims=True)
        spread = jnp.mean(center * center, axis=0, keepdims=True)
        ret[h * HEAD : (h + 1) * HEAD, :] = center * lax.rsqrt(spread + EPSILON)

    out = (ret[...].T * head_gain[...].astype(F32) * (gating * jax.nn.sigmoid(gating))).astype(BF16)
    out = out.reshape(TP, SHARE, 128)
    for z in range(Z):
        gated[z] = out
    for copy in out_copies:
        copy.wait()


def retain(tokens, states, wq, wk, wv, wg, mix_gain, head_gain, decays, cosine, sines):
    any_space = pl.BlockSpec(memory_space=pl.ANY)
    vmem = pl.BlockSpec(memory_space=pltpu.VMEM)
    return pl.pallas_call(
        retain_kernel,
        out_shape=(
            jax.ShapeDtypeStruct((2, HEAD, HEAD, ROWS), F32),
            jax.ShapeDtypeStruct((Z, TP, SHARE, 128), BF16),
        ),
        in_specs=[pl.BlockSpec(memory_space=pltpu.SMEM), vmem] + [any_space] * 5 + [vmem] * 4,
        out_specs=(any_space, vmem),
        scratch_shapes=[
            pltpu.VMEM((D, 512), BF16),
            pltpu.VMEM((2, HEAD, HEAD, ROWS), F32),
            pltpu.VMEM((2, HEAD, HEAD, ROWS), F32),
            pltpu.VMEM((128, ROWS), F32),
            pltpu.VMEM((128, ROWS), F32),
            pltpu.VMEM((128, ROWS), F32),
            pltpu.SemaphoreType.DMA((4,)),
            pltpu.SemaphoreType.DMA((CHUNKS,)),
            pltpu.SemaphoreType.DMA((CHUNKS,)),
        ],
        compiler_params=pltpu.CompilerParams(vmem_limit_bytes=40 * 2**20),
        name="retain",
    )(decays, tokens, states, wq, wk, wv, wg, mix_gain, head_gain, cosine, sines)


def mixer_kernel(*refs):
    gated, tokens, channel_gain, own_up, own_down = refs[:5]
    outs_mine, outs_other, packs = refs[5:9], refs[9], refs[10:16]
    out, heads, w_out, up, down, sems, o_sems = refs[16:]
    core = lax.axis_index("c")
    y = lax.axis_index("y")
    copies = []
    for k in range(Y):
        from_y = lax.rem(y + (Y - k), Y)
        copies.append(
            pltpu.make_async_copy(outs_mine[k], w_out.at[2 * from_y + core], o_sems.at[2 * k])
        )
        copies.append(
            pltpu.make_async_copy(
                outs_other.at[k], w_out.at[2 * from_y + (1 - core)], o_sems.at[2 * k + 1]
            )
        )
    up_copies = [pltpu.make_async_copy(own_up, up.at[:, :, pl.ds(0, 256)], sems.at[0])]
    down_copies = [
        pltpu.make_async_copy(
            own_down.at[:, pl.ds(256 * j, 256)], down.at[j, pl.ds(0, 256)], sems.at[1 + j]
        )
        for j in range(8)
    ]
    for p, packed in enumerate(packs):
        at = 256 + 128 * p
        for i in range(2):
            up_copies.append(
                pltpu.make_async_copy(
                    packed.at[pl.ds(0, 8), :, pl.ds(128 * i, 128)],
                    up.at[pl.ds(8 * i, 8), :, pl.ds(at, 128)],
                    sems.at[9 + 3 * p + i],
                )
            )
        down_copies.append(
            pltpu.make_async_copy(
                packed.at[pl.ds(8, 8)], down.at[:, pl.ds(at, 128), :], sems.at[9 + 3 * p + 2]
            )
        )
    for copy in copies + up_copies + down_copies:
        copy.start()
    for z in range(Z):
        for t in range(TP):
            heads[SHARE * z : SHARE * (z + 1), 128 * t : 128 * (t + 1)] = gated[z, t]
    for copy in copies:
        copy.wait()
    squares = jnp.zeros((ROWS, 256), F32)
    middle = []
    scaled = []
    for j in range(TP):
        at = slice(256 * j, 256 * j + 256)
        attended = jnp.dot(
            heads[...], w_out[:, :, at].reshape(1024, 256), preferred_element_type=F32
        )
        rounded = (tokens[:, j].reshape(ROWS, 256).astype(F32) + attended).astype(BF16)
        wide = rounded.astype(F32)
        squares += wide * wide
        middle.append(rounded)
        scaled.append((wide * channel_gain[:, at].astype(F32)).astype(BF16))
    second_rms = lax.rsqrt(jnp.sum(squares, axis=1, keepdims=True) / D + EPSILON)
    scaled = jnp.concatenate(scaled, axis=1)
    for copy in up_copies:
        copy.wait()
    activated = []
    for n in range(4):
        hidden = second_rms * jnp.dot(
            scaled,
            up[:, :, 256 * n : 256 * n + 256].reshape(D, 256),
            preferred_element_type=F32,
        )
        activated.append(jnp.square(jax.nn.relu(hidden)).astype(BF16))
    activated = jnp.concatenate(activated, axis=1)
    for copy in down_copies:
        copy.wait()
    row = lax.broadcasted_iota(jnp.int32, (ROWS, 1), 0)
    mine = row // SHARE == lax.axis_index("z")
    for j in range(TP):
        part = jnp.dot(activated, down[j], preferred_element_type=F32)
        part = part + jnp.where(mine, middle[j].astype(F32), 0.0)
        out[:, j] = part.astype(BF16).reshape(Z, SHARE, 256)


def mixer(gated, tokens, channel_gain, own_up, own_down, outs_mine, outs_other, packs):
    any_space = pl.BlockSpec(memory_space=pl.ANY)
    vmem = pl.BlockSpec(memory_space=pltpu.VMEM)
    return pl.pallas_call(
        mixer_kernel,
        out_shape=jax.ShapeDtypeStruct((Z, TP, SHARE, 256), BF16),
        in_specs=[vmem] * 3 + [any_space] * 13,
        out_specs=vmem,
        scratch_shapes=[
            pltpu.VMEM((ROWS, 1024), BF16),
            pltpu.VMEM((TP, 128, D), BF16),
            pltpu.VMEM((16, 128, 1024), BF16),
            pltpu.VMEM((8, 1024, 256), BF16),
            pltpu.SemaphoreType.DMA((27,)),
            pltpu.SemaphoreType.DMA((8,)),
        ],
        compiler_params=pltpu.CompilerParams(vmem_limit_bytes=40 * 2**20),
        name="mixer",
    )(gated, tokens, channel_gain, own_up.reshape(16, 128, 256), own_down,
      *outs_mine, outs_other, *packs)


def shift(count, by):
    return [(i, (i + by) % count) for i in range(count)]


def to_all(array, axes):
    return lax.all_to_all(array, axes, 0, 0, tiled=True)


def local(
    tokens, states, mix_gain, w_query, w_key, w_value, w_gate, head_gain, w_output,
    channel_gain, w_up, w_down,
):
    tp_index = lax.axis_index("y") * C + lax.axis_index("c")
    rows = to_all(jnp.broadcast_to(tokens[None], (TP, ROWS, 256)), ("y", "c"))
    packed = pack(w_up, w_down)
    near = [lax.ppermute(packed, "x", shift(X, by)) for by in (1, 3, 2)]
    outs = [w_output] + [lax.ppermute(w_output, "y", shift(Y, by)) for by in (1, 2, 3)]
    column = to_all(
        jnp.broadcast_to(
            tokens.reshape(1, TP, SHARE, 256), (Z, TP, SHARE, 256)
        ).reshape(Z * TP, SHARE, 256),
        ("z", "y", "c"),
    ).reshape(Z, TP, SHARE, 256)
    half = HEAD // 2
    frequency = ROTARY_BASE ** (-jnp.arange(half, dtype=F32) / half)
    angles = POS * frequency
    cosine = jnp.broadcast_to(jnp.cos(angles)[:, None], (half, ROWS))
    sines = jnp.broadcast_to(jnp.sin(angles)[:, None], (half, ROWS))
    head_ids = (tp_index * 2 + jnp.arange(2)).astype(F32)
    decays = 1.0 - jnp.exp2(-1.0 - 11.0 * head_ids / (HEADS - 1))
    new_states, gated = retain(
        rows, states.transpose(1, 2, 3, 0), w_query, w_key, w_value, w_gate,
        mix_gain.reshape(1, D), head_gain.reshape(1, 128), decays, cosine, sines,
    )
    gated = to_all(gated.reshape(Z * TP, SHARE, 128), ("z", "y", "c"))
    swap = [(0, 1), (1, 0)]
    outs_other = lax.ppermute(jnp.stack(outs), "c", swap)
    far = [lax.ppermute(p, "c", swap) for p in near]
    down = mixer(
        gated.reshape(Z, TP, SHARE, 128), column, channel_gain.reshape(1, D), w_up, w_down,
        outs, outs_other, near + far,
    )
    down = to_all(down.reshape(Z * TP, SHARE, 256), ("z", "y", "c"))
    layer_out = jnp.sum(down.reshape(Z, ROWS, 256).astype(F32), axis=0).astype(BF16)
    return (layer_out, new_states.transpose(3, 0, 1, 2))


def solution(mesh):
    torus = Mesh(mesh.devices.reshape(Z, X, Y, C), ("z", "x", "y", "c"))
    kv, tp = ("z", "x"), ("y", "c")
    in_specs = (
        P(kv, tp), P(kv, tp, None, None), P(), P(None, tp), P(None, tp), P(None, tp), P(None, tp),
        P(tp), P(tp, None), P(), P(None, kv), P(kv, None),
    )
    out_specs = (P(kv, tp), P(kv, tp, None, None))
    return jax.shard_map(local, mesh=torus, in_specs=in_specs, out_specs=out_specs, check_vma=False)
```

```python
import jax
import jax.numpy as jnp
import numpy as np
from jax import lax
from jax.experimental import pallas as pl
from jax.experimental.pallas import tpu as pltpu
from jax.sharding import Mesh
from jax.sharding import PartitionSpec as P


HEADS = 16
HEAD = 64
POS = 16384
D = 2048
EPSILON = 1e-06
ROTARY_BASE = 10000.0
ROWS = 128
Z, X, Y, C = 8, 4, 4, 2
TP = Y * C
SHARE = ROWS // TP
RETAIN_LIMIT = 58 * 2**20
MIXER_LIMIT = 40 * 2**20
F32 = jnp.float32
BF16 = jnp.bfloat16


def copy_all(copies):
    for copy in copies:
        copy.start()
    for copy in copies:
        copy.wait()


def pack_kernel(up, down, packed, sems):
    at = pl.multiple_of(lax.axis_index("c") * 128, 128)
    copies = [
        pltpu.make_async_copy(
            up.at[pl.ds(8 * i, 8), :, pl.ds(at, 128)],
            packed.at[pl.ds(0, 8), :, pl.ds(128 * i, 128)],
            sems.at[i],
        )
        for i in range(2)
    ]
    copies += [
        pltpu.make_async_copy(
            down.at[pl.ds(at, 128), pl.ds(256 * j, 256)], packed.at[8 + j], sems.at[2 + j]
        )
        for j in range(8)
    ]
    copy_all(copies)


def pack(w_up, w_down):
    return pl.pallas_call(
        pack_kernel,
        out_shape=jax.ShapeDtypeStruct((16, 128, 256), BF16),
        in_specs=[pl.BlockSpec(memory_space=pltpu.HBM)] * 2,
        out_specs=pl.BlockSpec(memory_space=pltpu.VMEM),
        scratch_shapes=[pltpu.SemaphoreType.DMA((10,))],
        name="pack",
    )(w_up.reshape(16, 128, 256), w_down)


CHUNKS = 8
PER_HEAD = CHUNKS // 2
STEP = HEAD // PER_HEAD
ANGLES = POS * ROTARY_BASE ** (-np.arange(HEAD // 2) / (HEAD // 2))
COSINE = np.broadcast_to(np.cos(ANGLES)[:, None], (HEAD // 2, ROWS)).astype(np.float32)
SINES = np.broadcast_to(np.sin(ANGLES)[:, None], (HEAD // 2, ROWS)).astype(np.float32)
DECAYS = (1.0 - 2.0 ** (-1.0 - 11.0 * np.arange(HEADS) / (HEADS - 1))).astype(np.float32)


def gain_row(gain, j):
    wide = gain[...].astype(F32)
    return jnp.concatenate([wide[2 * j : 2 * j + 1], wide[2 * j + 1 : 2 * j + 2]], axis=1)


def retain_kernel(
    decays, tokens, states, wq, wk, wv, wg, wo, mix_gain, head_gain, cosine, sines,
    new_states, partial, weights, w_out, old, new, qt, kt, ret, w_sems, in_sems, out_sems,
):
    def part(ref, i):
        return ref.at[i // PER_HEAD, pl.ds((i % PER_HEAD) * STEP, STEP)]

    first_head = 2 * (lax.axis_index("y") * C + lax.axis_index("c"))
    w_copies = [
        pltpu.make_async_copy(w, weights.at[:, pl.ds(128 * i, 128)], w_sems.at[i])
        for i, w in enumerate((wq, wk, wv, wg))
    ]
    wo_copy = pltpu.make_async_copy(wo, w_out, w_sems.at[4])
    in_copies = [
        pltpu.make_async_copy(part(states, i), part(old, i), in_sems.at[i]) for i in range(CHUNKS)
    ]
    out_copies = [
        pltpu.make_async_copy(part(new, i), part(new_states, i), out_sems.at[i])
        for i in range(CHUNKS)
    ]
    for copy in w_copies + in_copies + [wo_copy]:
        copy.start()

    squares = jnp.zeros((ROWS, 256), F32)
    for j in range(TP):
        block = tokens[j].astype(F32)
        squares += block * block
    inverse_rms = lax.rsqrt(jnp.sum(squares, axis=1, keepdims=True) / D + EPSILON)
    normed = jnp.concatenate(
        [
            (tokens[j].astype(F32) * inverse_rms * gain_row(mix_gain, j)).astype(BF16)
            for j in range(TP)
        ],
        axis=1,
    )
    for copy in w_copies:
        copy.wait()
    projected = jnp.dot(normed, weights[...], preferred_element_type=F32)
    half = HEAD // 2

    def turned(flat):
        rows = []
        for h in range(2):
            a = flat[h * HEAD : h * HEAD + half]
            b = flat[h * HEAD + half : (h + 1) * HEAD]
            rows += [a * cosine[...] - b * sines[...], a * sines[...] + b * cosine[...]]
        return jnp.concatenate(rows, axis=0)

    qt[...] = turned(projected[:, 0:128].T) * HEAD**-0.5
    kt[...] = turned(projected[:, 128:256].T)
    vt = projected[:, 256:384].T
    gating = projected[:, 384:512]

    for h in range(2):
        values = vt[h * HEAD : (h + 1) * HEAD]
        decay = decays[first_head + h]
        total = jnp.zeros((HEAD, ROWS), F32)
        for i in range(h * PER_HEAD, (h + 1) * PER_HEAD):
            in_copies[i].wait()
            first = (i % PER_HEAD) * STEP

            def step(s, total):
                k = first + s
                row = h * HEAD + k
                fresh = decay * old[h, k] + kt[pl.ds(row, 1), :] * values
                new[h, k] = fresh
                return total + qt[pl.ds(row, 1), :] * fresh

            total = lax.fori_loop(0, STEP, step, total, unroll=8)
            out_copies[i].start()
        center = total - jnp.mean(total, axis=0, keepdims=True)
        spread = jnp.mean(center * center, axis=0, keepdims=True)
        ret[h * HEAD : (h + 1) * HEAD, :] = center * lax.rsqrt(spread + EPSILON)

    out = (ret[...].T * head_gain[...].astype(F32) * (gating * jax.nn.sigmoid(gating))).astype(BF16)
    wo_copy.wait()
    partial[...] = (
        jnp.dot(out, w_out[...], preferred_element_type=F32).astype(BF16).reshape(TP, SHARE, D)
    )
    for copy in out_copies:
        copy.wait()


def retain(tokens, states, wq, wk, wv, wg, wo, mix_gain, head_gain):
    any_space = pl.BlockSpec(memory_space=pl.ANY)
    vmem = pl.BlockSpec(memory_space=pltpu.VMEM)
    return pl.pallas_call(
        retain_kernel,
        out_shape=(
            jax.ShapeDtypeStruct((2, HEAD, HEAD, ROWS), F32),
            jax.ShapeDtypeStruct((TP, SHARE, D), BF16),
        ),
        in_specs=[pl.BlockSpec(memory_space=pltpu.SMEM), vmem] + [any_space] * 6 + [vmem] * 4,
        out_specs=(any_space, vmem),
        scratch_shapes=[
            pltpu.VMEM((D, 512), BF16),
            pltpu.VMEM((128, D), BF16),
            pltpu.VMEM((2, HEAD, HEAD, ROWS), F32),
            pltpu.VMEM((2, HEAD, HEAD, ROWS), F32),
            pltpu.VMEM((128, ROWS), F32),
            pltpu.VMEM((128, ROWS), F32),
            pltpu.VMEM((128, ROWS), F32),
            pltpu.SemaphoreType.DMA((5,)),
            pltpu.SemaphoreType.DMA((CHUNKS,)),
            pltpu.SemaphoreType.DMA((CHUNKS,)),
        ],
        compiler_params=pltpu.CompilerParams(vmem_limit_bytes=RETAIN_LIMIT),
        name="retain",
    )(
        DECAYS, tokens, states, wq, wk, wv, wg, wo, mix_gain.reshape(16, 128),
        head_gain.reshape(1, 128), COSINE, SINES,
    )


def middle_kernel(parts, tokens, out):
    at = pl.multiple_of((lax.axis_index("y") * C + lax.axis_index("c")) * SHARE, SHARE)
    total = parts[0].astype(F32)
    for t in range(1, TP):
        total += parts[t].astype(F32)
    own = jnp.concatenate([tokens[j, pl.ds(at, SHARE), :] for j in range(TP)], axis=1)
    middle = (own.astype(F32) + total).astype(BF16)
    for z in range(Z):
        out[z] = middle


def middle_rows(parts, tokens):
    vmem = pl.BlockSpec(memory_space=pltpu.VMEM)
    return pl.pallas_call(
        middle_kernel,
        out_shape=jax.ShapeDtypeStruct((Z, SHARE, D), BF16),
        in_specs=[vmem] * 2,
        out_specs=vmem,
        compiler_params=pltpu.CompilerParams(vmem_limit_bytes=8 * 2**20),
        name="middle",
    )(parts, tokens)


def mixer_kernel(*refs):
    rows, channel_gain, own_up, own_down = refs[:4]
    ups, downs = refs[4:10], refs[10:16]
    out, up, down, sems = refs[16:]
    up_copies = [pltpu.make_async_copy(own_up, up.at[:, :, pl.ds(0, 256)], sems.at[0])]
    down_copies = [
        pltpu.make_async_copy(
            own_down.at[:, pl.ds(256 * j, 256)], down.at[j, pl.ds(0, 256)], sems.at[1 + j]
        )
        for j in range(8)
    ]
    for p in range(6):
        at = 256 + 128 * p
        for i in range(2):
            up_copies.append(
                pltpu.make_async_copy(
                    ups[p].at[pl.ds(0, 8), :, pl.ds(128 * i, 128)],
                    up.at[pl.ds(8 * i, 8), :, pl.ds(at, 128)],
                    sems.at[9 + 3 * p + i],
                )
            )
        last = downs[p].shape[0] - 8
        down_copies.append(
            pltpu.make_async_copy(
                downs[p].at[pl.ds(last, 8)], down.at[:, pl.ds(at, 128), :], sems.at[9 + 3 * p + 2]
            )
        )
    for copy in up_copies + down_copies:
        copy.start()
    squares = jnp.zeros((ROWS, 256), F32)
    scaled = []
    for j in range(TP):
        wide = rows[:, :, 256 * j : 256 * j + 256].reshape(ROWS, 256).astype(F32)
        squares += wide * wide
        scaled.append((wide * gain_row(channel_gain, j)).astype(BF16))
    second_rms = lax.rsqrt(jnp.sum(squares, axis=1, keepdims=True) / D + EPSILON)
    scaled = jnp.concatenate(scaled, axis=1)
    activated = []
    for n in range(4):
        for copy in up_copies[0:1] if n == 0 else up_copies[4 * n - 3 : 4 * n + 1]:
            copy.wait()
        hidden = second_rms * jnp.dot(
            scaled,
            up[:, :, 256 * n : 256 * n + 256].reshape(D, 256),
            preferred_element_type=F32,
        )
        activated.append(jnp.square(jax.nn.relu(hidden)).astype(BF16))
    activated = jnp.concatenate(activated, axis=1)
    for copy in down_copies:
        copy.wait()
    row = lax.broadcasted_iota(jnp.int32, (ROWS, 1), 0)
    mine = row // SHARE == lax.axis_index("z")
    for j in range(TP):
        part = jnp.dot(activated, down[j], preferred_element_type=F32)
        own = rows[:, :, 256 * j : 256 * j + 256].reshape(ROWS, 256).astype(F32)
        part = part + jnp.where(mine, own, 0.0)
        out[:, j] = part.astype(BF16).reshape(Z, SHARE, 256)


def mixer(rows, channel_gain, own_up, own_down, ups, downs):
    any_space = pl.BlockSpec(memory_space=pl.ANY)
    vmem = pl.BlockSpec(memory_space=pltpu.VMEM)
    return pl.pallas_call(
        mixer_kernel,
        out_shape=jax.ShapeDtypeStruct((Z, TP, SHARE, 256), BF16),
        in_specs=[vmem] * 2 + [any_space] * 14,
        out_specs=vmem,
        scratch_shapes=[
            pltpu.VMEM((16, 128, 1024), BF16),
            pltpu.VMEM((8, 1024, 256), BF16),
            pltpu.SemaphoreType.DMA((27,)),
        ],
        compiler_params=pltpu.CompilerParams(vmem_limit_bytes=MIXER_LIMIT),
        name="mixer",
    )(rows, channel_gain.reshape(16, 128), own_up.reshape(16, 128, 256), own_down, *ups, *downs)


def shift(count, by):
    return [(i, (i + by) % count) for i in range(count)]


def to_all(array, axes):
    return lax.all_to_all(array, axes, 0, 0, tiled=True)


def local(
    tokens, states, mix_gain, w_query, w_key, w_value, w_gate, head_gain, w_output,
    channel_gain, w_up, w_down,
):
    rows = to_all(jnp.broadcast_to(tokens[None], (TP, ROWS, 256)), ("y", "c"))
    packed = pack(w_up, w_down)
    left = lax.ppermute(packed, "x", shift(X, 1))
    right = lax.ppermute(packed, "x", shift(X, 3))
    new_states, partial = retain(
        rows, states.transpose(1, 2, 3, 0), w_query, w_key, w_value, w_gate, w_output,
        mix_gain, head_gain,
    )
    parts = to_all(partial, ("y", "c"))
    far_up = lax.ppermute(left[:8], "x", shift(X, 1))
    far_down = lax.ppermute(right[8:], "x", shift(X, 3))
    middle = middle_rows(parts, rows)
    everyone = to_all(middle, "z")
    swap = [(0, 1), (1, 0)]
    left_other = lax.ppermute(left, "c", swap)
    right_other = lax.ppermute(right, "c", swap)
    up_other = lax.ppermute(far_up, "c", swap)
    down_other = lax.ppermute(far_down, "c", swap)
    down = mixer(
        everyone, channel_gain, w_up, w_down,
        (left, left_other, right, right_other, far_up, up_other),
        (left, left_other, right, right_other, far_down, down_other),
    )
    down = to_all(down.reshape(Z * TP, SHARE, 256), ("z", "y", "c"))
    layer_out = jnp.sum(down.reshape(Z, ROWS, 256).astype(F32), axis=0).astype(BF16)
    return (layer_out, new_states.transpose(3, 0, 1, 2))


def solution(mesh):
    torus = Mesh(mesh.devices.reshape(Z, X, Y, C), ("z", "x", "y", "c"))
    kv, tp = ("z", "x"), ("y", "c")
    in_specs = (
        P(kv, tp), P(kv, tp, None, None), P(), P(None, tp), P(None, tp), P(None, tp), P(None, tp),
        P(tp), P(tp, None), P(), P(None, kv), P(kv, None),
    )
    out_specs = (P(kv, tp), P(kv, tp, None, None))
    return jax.shard_map(local, mesh=torus, in_specs=in_specs, out_specs=out_specs, check_vma=False)
```

```python
import jax
import jax.numpy as jnp
import numpy as np
from jax import lax
from jax.experimental import pallas as pl
from jax.experimental.pallas import tpu as pltpu
from jax.sharding import Mesh
from jax.sharding import PartitionSpec as P


HEADS = 16
HEAD = 64
POS = 16384
D = 2048
EPSILON = 1e-06
ROTARY_BASE = 10000.0
ROWS = 128
Z, X, Y, C = 8, 4, 4, 2
TP = Y * C
SHARE = ROWS // TP
RETAIN_LIMIT = 20 * 2**20
MIXER_LIMIT = 20 * 2**20
F32 = jnp.float32
BF16 = jnp.bfloat16


def in_hbm(array):
    return pltpu.with_memory_space_constraint(array, pltpu.HBM)


def in_vmem(array):
    return pltpu.with_memory_space_constraint(array, pltpu.VMEM)


def copy_all(copies):
    for copy in copies:
        copy.start()
    for copy in copies:
        copy.wait()


def pack_kernel(up, down, packed, sems):
    at = pl.multiple_of(lax.axis_index("c") * 128, 128)
    copies = [
        pltpu.make_async_copy(
            up.at[pl.ds(8 * i, 8), :, pl.ds(at, 128)],
            packed.at[pl.ds(0, 8), :, pl.ds(128 * i, 128)],
            sems.at[i],
        )
        for i in range(2)
    ]
    copies += [
        pltpu.make_async_copy(
            down.at[pl.ds(at, 128), pl.ds(256 * j, 256)], packed.at[8 + j], sems.at[2 + j]
        )
        for j in range(8)
    ]
    copy_all(copies)


def pack(w_up, w_down):
    return pl.pallas_call(
        pack_kernel,
        out_shape=jax.ShapeDtypeStruct((16, 128, 256), BF16),
        in_specs=[pl.BlockSpec(memory_space=pl.ANY)] * 2,
        out_specs=pl.BlockSpec(memory_space=pltpu.VMEM),
        scratch_shapes=[pltpu.SemaphoreType.DMA((10,))],
        compiler_params=pltpu.CompilerParams(vmem_limit_bytes=8 * 2**20),
        name="pack",
    )(in_hbm(w_up.reshape(16, 128, 256)), in_hbm(w_down))


CHUNKS = 8
PER_HEAD = CHUNKS // 2
STEP = HEAD // PER_HEAD
ANGLES = POS * ROTARY_BASE ** (-np.arange(HEAD // 2) / (HEAD // 2))
COSINE = np.broadcast_to(np.cos(ANGLES)[:, None], (HEAD // 2, ROWS)).astype(np.float32)
SINES = np.broadcast_to(np.sin(ANGLES)[:, None], (HEAD // 2, ROWS)).astype(np.float32)
DECAYS = (1.0 - 2.0 ** (-1.0 - 11.0 * np.arange(HEADS) / (HEADS - 1))).astype(np.float32)


def gain_row(gain, j):
    wide = gain[...].astype(F32)
    return jnp.concatenate([wide[2 * j : 2 * j + 1], wide[2 * j + 1 : 2 * j + 2]], axis=1)


def place(k, other):
    y, c = lax.axis_index("y"), lax.axis_index("c")
    return 2 * lax.rem(y + (Y - k), Y) + (1 - c if other else c)


def retain_kernel(decays, *refs):
    blocks = refs[:TP]
    states, wq, wk, wv, wg, wo, mix_gain, head_gain, cosine, sines = refs[TP : TP + 10]
    new_states, mine, others, own = refs[TP + 10 : TP + 14]
    tokens, weights, w_out, old, new, qt, kt, ret, shares = refs[TP + 14 : TP + 23]
    w_sems, in_sems, out_sems = refs[TP + 23 :]

    def part(ref, i):
        return ref.at[i // PER_HEAD, pl.ds((i % PER_HEAD) * STEP, STEP)]

    first_head = 2 * (lax.axis_index("y") * C + lax.axis_index("c"))
    w_copies = [
        pltpu.make_async_copy(w, weights.at[:, pl.ds(128 * i, 128)], w_sems.at[i])
        for i, w in enumerate((wq, wk, wv, wg))
    ]
    wo_copy = pltpu.make_async_copy(wo, w_out, w_sems.at[4])
    in_copies = [
        pltpu.make_async_copy(part(states, i), part(old, i), in_sems.at[i]) for i in range(CHUNKS)
    ]
    out_copies = [
        pltpu.make_async_copy(part(new, i), part(new_states, i), out_sems.at[i])
        for i in range(CHUNKS)
    ]
    for copy in w_copies + in_copies + [wo_copy]:
        copy.start()

    squares = jnp.zeros((ROWS, 256), F32)
    for i in range(TP):
        block = blocks[i][...]
        tokens[place(i % Y, i >= Y)] = block
        block = block.astype(F32)
        squares += block * block
    inverse_rms = lax.rsqrt(jnp.sum(squares, axis=1, keepdims=True) / D + EPSILON)
    normed = jnp.concatenate(
        [
            (tokens[j].astype(F32) * inverse_rms * gain_row(mix_gain, j)).astype(BF16)
            for j in range(TP)
        ],
        axis=1,
    )
    for copy in w_copies:
        copy.wait()
    projected = jnp.dot(normed, weights[...], preferred_element_type=F32)
    half = HEAD // 2

    def turned(flat):
        rows = []
        for h in range(2):
            a = flat[h * HEAD : h * HEAD + half]
            b = flat[h * HEAD + half : (h + 1) * HEAD]
            rows += [a * cosine[...] - b * sines[...], a * sines[...] + b * cosine[...]]
        return jnp.concatenate(rows, axis=0)

    qt[...] = turned(projected[:, 0:128].T) * HEAD**-0.5
    kt[...] = turned(projected[:, 128:256].T)
    vt = projected[:, 256:384].T
    gating = projected[:, 384:512]

    for h in range(2):
        values = vt[h * HEAD : (h + 1) * HEAD]
        decay = decays[first_head + h]
        total = jnp.zeros((HEAD, ROWS), F32)
        for i in range(h * PER_HEAD, (h + 1) * PER_HEAD):
            in_copies[i].wait()
            first = (i % PER_HEAD) * STEP

            def step(s, total):
                k = first + s
                row = h * HEAD + k
                fresh = decay * old[h, k] + kt[pl.ds(row, 1), :] * values
                new[h, k] = fresh
                return total + qt[pl.ds(row, 1), :] * fresh

            total = lax.fori_loop(0, STEP, step, total, unroll=8)
            out_copies[i].start()
        center = total - jnp.mean(total, axis=0, keepdims=True)
        spread = jnp.mean(center * center, axis=0, keepdims=True)
        ret[h * HEAD : (h + 1) * HEAD, :] = center * lax.rsqrt(spread + EPSILON)

    out = (ret[...].T * head_gain[...].astype(F32) * (gating * jax.nn.sigmoid(gating))).astype(BF16)
    wo_copy.wait()
    partial = jnp.dot(out, w_out[...], preferred_element_type=F32)
    shares[...] = partial.reshape(Y, C, SHARE, D)
    core = lax.axis_index("c")
    mine[...] = shares[:, core]
    others[...] = shares[:, 1 - core].astype(BF16)
    at = pl.multiple_of(place(0, False) * SHARE, SHARE)
    own[...] = jnp.concatenate([tokens[j, pl.ds(at, SHARE), :] for j in range(TP)], axis=1)
    for copy in out_copies:
        copy.wait()


def retain(blocks, states, wq, wk, wv, wg, wo, mix_gain, head_gain):
    any_space = pl.BlockSpec(memory_space=pl.ANY)
    vmem = pl.BlockSpec(memory_space=pltpu.VMEM)
    return pl.pallas_call(
        retain_kernel,
        out_shape=(
            jax.ShapeDtypeStruct((2, HEAD, HEAD, ROWS), F32),
            jax.ShapeDtypeStruct((Y, SHARE, D), F32),
            jax.ShapeDtypeStruct((Y, SHARE, D), BF16),
            jax.ShapeDtypeStruct((SHARE, D), BF16),
        ),
        in_specs=[pl.BlockSpec(memory_space=pltpu.SMEM)]
        + [vmem] * TP + [any_space] * 6 + [vmem] * 4,
        out_specs=(any_space, vmem, vmem, vmem),
        scratch_shapes=[
            pltpu.VMEM((TP, ROWS, 256), BF16),
            pltpu.VMEM((D, 512), BF16),
            pltpu.VMEM((128, D), BF16),
            pltpu.VMEM((2, HEAD, HEAD, ROWS), F32),
            pltpu.VMEM((2, HEAD, HEAD, ROWS), F32),
            pltpu.VMEM((128, ROWS), F32),
            pltpu.VMEM((128, ROWS), F32),
            pltpu.VMEM((128, ROWS), F32),
            pltpu.VMEM((Y, C, SHARE, D), F32),
            pltpu.SemaphoreType.DMA((5,)),
            pltpu.SemaphoreType.DMA((CHUNKS,)),
            pltpu.SemaphoreType.DMA((CHUNKS,)),
        ],
        compiler_params=pltpu.CompilerParams(vmem_limit_bytes=RETAIN_LIMIT),
        name="retain",
    )(
        in_hbm(DECAYS), in_hbm(blocks[0]), *map(in_vmem, blocks[1:]), *map(in_hbm, (states, wq, wk, wv, wg, wo)),
        *map(in_hbm, (mix_gain.reshape(16, 128), head_gain.reshape(1, 128), COSINE, SINES)),
    )


def pair_kernel(mine, others, *outs):
    y = lax.axis_index("y")
    for k in range(Y):
        to = lax.rem(y + k, Y)
        outs[k][...] = (mine[to] + others[to].astype(F32)).astype(outs[k].dtype)


def pair(mine, others):
    vmem = pl.BlockSpec(memory_space=pltpu.VMEM)
    return pl.pallas_call(
        pair_kernel,
        out_shape=[jax.ShapeDtypeStruct((SHARE, D), BF16 if k else F32) for k in range(Y)],
        in_specs=[vmem] * 2,
        out_specs=[vmem] * Y,
        compiler_params=pltpu.CompilerParams(vmem_limit_bytes=8 * 2**20),
        name="pair",
    )(in_vmem(mine), in_vmem(others))


def middle_kernel(own, first, *refs):
    total = first[...]
    for part in refs[:-1]:
        total += part[...].astype(F32)
    middle = (own[...].astype(F32) + total).astype(BF16)
    for z in range(Z):
        refs[-1][z] = middle


def middle_rows(own, parts):
    vmem = pl.BlockSpec(memory_space=pltpu.VMEM)
    return pl.pallas_call(
        middle_kernel,
        out_shape=jax.ShapeDtypeStruct((Z, SHARE, D), BF16),
        in_specs=[vmem] * (Y + 1),
        out_specs=vmem,
        compiler_params=pltpu.CompilerParams(vmem_limit_bytes=8 * 2**20),
        name="middle",
    )(*map(in_vmem, (own, *parts)))


def mixer_kernel(*refs):
    rows, channel_gain, own_up, own_down = refs[:4]
    ups, downs = refs[4:10], refs[10:16]
    out, up, down, sems = refs[16:]
    up_copies = [pltpu.make_async_copy(own_up, up.at[:, :, pl.ds(0, 256)], sems.at[0])]
    down_copies = [
        pltpu.make_async_copy(
            own_down.at[:, pl.ds(256 * j, 256)], down.at[j, pl.ds(0, 256)], sems.at[1 + j]
        )
        for j in range(8)
    ]
    for p in range(6):
        at = 256 + 128 * p
        for i in range(2):
            up_copies.append(
                pltpu.make_async_copy(
                    ups[p].at[pl.ds(0, 8), :, pl.ds(128 * i, 128)],
                    up.at[pl.ds(8 * i, 8), :, pl.ds(at, 128)],
                    sems.at[9 + 3 * p + i],
                )
            )
        down_copies.append(
            pltpu.make_async_copy(
                downs[p].at[pl.ds(downs[p].shape[0] - 8, 8)],
                down.at[:, pl.ds(at, 128), :],
                sems.at[9 + 3 * p + 2],
            )
        )
    for copy in up_copies + down_copies:
        copy.start()
    squares = jnp.zeros((ROWS, 256), F32)
    scaled = []
    for j in range(TP):
        wide = rows[:, :, 256 * j : 256 * j + 256].reshape(ROWS, 256).astype(F32)
        squares += wide * wide
        scaled.append((wide * gain_row(channel_gain, j)).astype(BF16))
    second_rms = lax.rsqrt(jnp.sum(squares, axis=1, keepdims=True) / D + EPSILON)
    scaled = jnp.concatenate(scaled, axis=1)
    activated = []
    for n in range(4):
        for copy in up_copies[0:1] if n == 0 else up_copies[4 * n - 3 : 4 * n + 1]:
            copy.wait()
        hidden = second_rms * jnp.dot(
            scaled,
            up[:, :, 256 * n : 256 * n + 256].reshape(D, 256),
            preferred_element_type=F32,
        )
        activated.append(jnp.square(jax.nn.relu(hidden)).astype(BF16))
    activated = jnp.concatenate(activated, axis=1)
    for copy in down_copies:
        copy.wait()
    row = lax.broadcasted_iota(jnp.int32, (ROWS, 1), 0)
    mine = row // SHARE == lax.axis_index("z")
    for j in range(TP):
        part = jnp.dot(activated, down[j], preferred_element_type=F32)
        own = rows[:, :, 256 * j : 256 * j + 256].reshape(ROWS, 256).astype(F32)
        part = part + jnp.where(mine, own, 0.0)
        out[:, j] = part.astype(BF16).reshape(Z, SHARE, 256)


def mixer(rows, channel_gain, own_up, own_down, ups, downs):
    any_space = pl.BlockSpec(memory_space=pl.ANY)
    vmem = pl.BlockSpec(memory_space=pltpu.VMEM)
    return pl.pallas_call(
        mixer_kernel,
        out_shape=pltpu.VMEM((Z, TP, SHARE, 256), BF16),
        in_specs=[vmem] * 2 + [any_space] * 14,
        out_specs=vmem,
        scratch_shapes=[
            pltpu.VMEM((16, 128, 1024), BF16),
            pltpu.VMEM((8, 1024, 256), BF16),
            pltpu.SemaphoreType.DMA((27,)),
        ],
        compiler_params=pltpu.CompilerParams(vmem_limit_bytes=MIXER_LIMIT),
        name="mixer",
    )(
        in_vmem(rows), in_hbm(channel_gain.reshape(16, 128)), in_hbm(own_up.reshape(16, 128, 256)),
        in_hbm(own_down), *map(in_hbm, ups), *map(in_hbm, downs),
    )


def shift(count, by):
    return [(i, (i + by) % count) for i in range(count)]


def to_all(array, axes):
    return lax.all_to_all(array, axes, 0, 0, tiled=True)


def local(
    tokens, states, mix_gain, w_query, w_key, w_value, w_gate, head_gain, w_output,
    channel_gain, w_up, w_down,
):
    swap = [(0, 1), (1, 0)]
    blocks = [tokens] + [lax.ppermute(tokens, "y", shift(Y, by)) for by in (1, 2, 3)]
    packed = pack(w_up, w_down)
    left = lax.ppermute(packed, "x", shift(X, 1))
    right = lax.ppermute(packed, "x", shift(X, 3))
    blocks += [lax.ppermute(block, "c", swap) for block in blocks]
    new_states, mine, others, own = retain(
        blocks, states.transpose(1, 2, 3, 0), w_query, w_key, w_value, w_gate, w_output,
        mix_gain, head_gain,
    )
    others = lax.ppermute(others, "c", swap)
    parts = pair(mine, others)
    parts = [parts[0]] + [lax.ppermute(parts[k], "y", shift(Y, k)) for k in (1, 2, 3)]
    middle = middle_rows(own, parts)
    everyone = to_all(middle, "z")
    far_up = lax.ppermute(left[:8], "x", shift(X, 1))
    far_down = lax.ppermute(right[8:], "x", shift(X, 3))
    left_other, right_other = [lax.ppermute(w, "c", swap) for w in (left, right)]
    far_other = [lax.ppermute(w, "c", swap) for w in (far_up, far_down)]
    down = mixer(
        everyone, channel_gain, w_up, w_down,
        (left, left_other, right, right_other, far_up, far_other[0]),
        (left, left_other, right, right_other, far_down, far_other[1]),
    )
    down = to_all(down.reshape(Z * TP, SHARE, 256), ("z", "y", "c"))
    layer_out = jnp.sum(down.reshape(Z, ROWS, 256).astype(F32), axis=0).astype(BF16)
    return (layer_out, new_states.transpose(3, 0, 1, 2))


def solution(mesh):
    torus = Mesh(mesh.devices.reshape(Z, X, Y, C), ("z", "x", "y", "c"))
    kv, tp = ("z", "x"), ("y", "c")
    in_specs = (
        P(kv, tp), P(kv, tp, None, None), P(), P(None, tp), P(None, tp), P(None, tp), P(None, tp),
        P(tp), P(tp, None), P(), P(None, kv), P(kv, None),
    )
    out_specs = (P(kv, tp), P(kv, tp, None, None))
    return jax.shard_map(local, mesh=torus, in_specs=in_specs, out_specs=out_specs, check_vma=False)
```

```python
import jax
import jax.numpy as jnp
import numpy as np
from jax import lax
from jax.experimental import pallas as pl
from jax.experimental.pallas import tpu as pltpu
from jax.sharding import Mesh
from jax.sharding import PartitionSpec as P


HEADS = 16
HEAD = 64
POS = 16384
D = 2048
EPSILON = 1e-06
ROTARY_BASE = 10000.0
ROWS = 128
Z, X, Y, C = 8, 4, 4, 2
TP = Y * C
SHARE = ROWS // TP
RETAIN_LIMIT = 14 * 2**20
MIXER_LIMIT = 14 * 2**20
F32 = jnp.float32
BF16 = jnp.bfloat16


def in_hbm(array):
    return pltpu.with_memory_space_constraint(array, pltpu.HBM)


def in_vmem(array):
    return pltpu.with_memory_space_constraint(array, pltpu.VMEM)


def copy_all(copies):
    for copy in copies:
        copy.start()
    for copy in copies:
        copy.wait()


def pack_kernel(up, down, packed_up, packed_down, sems):
    at = pl.multiple_of(lax.axis_index("c") * 128, 128)
    copies = [
        pltpu.make_async_copy(
            up.at[pl.ds(8 * i, 8), :, pl.ds(at, 128)],
            packed_up.at[:, :, pl.ds(128 * i, 128)],
            sems.at[i],
        )
        for i in range(2)
    ]
    copies += [
        pltpu.make_async_copy(
            down.at[pl.ds(at, 128), pl.ds(256 * j, 256)], packed_down.at[j], sems.at[2 + j]
        )
        for j in range(8)
    ]
    copy_all(copies)


def pack(w_up, w_down):
    return pl.pallas_call(
        pack_kernel,
        out_shape=[jax.ShapeDtypeStruct((8, 128, 256), BF16)] * 2,
        in_specs=[pl.BlockSpec(memory_space=pl.ANY)] * 2,
        out_specs=[pl.BlockSpec(memory_space=pltpu.VMEM)] * 2,
        scratch_shapes=[pltpu.SemaphoreType.DMA((10,))],
        compiler_params=pltpu.CompilerParams(vmem_limit_bytes=8 * 2**20),
        name="pack",
    )(in_hbm(w_up.reshape(16, 128, 256)), in_hbm(w_down))


CHUNKS = 8
PER_HEAD = CHUNKS // 2
STEP = HEAD // PER_HEAD
ANGLES = POS * ROTARY_BASE ** (-np.arange(HEAD // 2) / (HEAD // 2))
COSINE = np.broadcast_to(np.cos(ANGLES)[:, None], (HEAD // 2, ROWS)).astype(np.float32)
SINES = np.broadcast_to(np.sin(ANGLES)[:, None], (HEAD // 2, ROWS)).astype(np.float32)
DECAYS = (1.0 - 2.0 ** (-1.0 - 11.0 * np.arange(HEADS) / (HEADS - 1))).astype(np.float32)


def gain_row(gain, j):
    wide = gain[...].astype(F32)
    return jnp.concatenate([wide[2 * j : 2 * j + 1], wide[2 * j + 1 : 2 * j + 2]], axis=1)


def place(k, other):
    y, c = lax.axis_index("y"), lax.axis_index("c")
    return 2 * lax.rem(y + (Y - k), Y) + (1 - c if other else c)


def part(ref, i):
    return ref.at[i // PER_HEAD, pl.ds((i % PER_HEAD) * STEP, STEP)]


def retain_kernel(decays, *refs):
    blocks = refs[:TP]
    states, wq, wk, wv, wg, wo, mix_gain, head_gain, cosine, sines = refs[TP : TP + 10]
    mine, others, own, keys, values = refs[TP + 10 : TP + 15]
    tokens, weights, w_out, old, qt, ret, shares = refs[TP + 15 : TP + 22]
    w_sems, in_sems = refs[TP + 22 :]

    first_head = 2 * (lax.axis_index("y") * C + lax.axis_index("c"))
    w_copies = [
        pltpu.make_async_copy(w, weights.at[:, pl.ds(128 * i, 128)], w_sems.at[i])
        for i, w in enumerate((wq, wk, wv, wg))
    ]
    wo_copy = pltpu.make_async_copy(wo, w_out, w_sems.at[4])
    in_copies = [
        pltpu.make_async_copy(part(states, i), part(old, i), in_sems.at[i]) for i in range(CHUNKS)
    ]
    for copy in w_copies + in_copies + [wo_copy]:
        copy.start()

    squares = jnp.zeros((ROWS, 256), F32)
    for i in range(TP):
        block = blocks[i][...]
        tokens[place(i % Y, i >= Y)] = block
        block = block.astype(F32)
        squares += block * block
    inverse_rms = lax.rsqrt(jnp.sum(squares, axis=1, keepdims=True) / D + EPSILON)
    normed = jnp.concatenate(
        [
            (tokens[j].astype(F32) * inverse_rms * gain_row(mix_gain, j)).astype(BF16)
            for j in range(TP)
        ],
        axis=1,
    )
    for copy in w_copies:
        copy.wait()
    projected = jnp.dot(normed, weights[...], preferred_element_type=F32)
    half = HEAD // 2

    def turned(flat):
        rows = []
        for h in range(2):
            a = flat[h * HEAD : h * HEAD + half]
            b = flat[h * HEAD + half : (h + 1) * HEAD]
            rows += [a * cosine[...] - b * sines[...], a * sines[...] + b * cosine[...]]
        return jnp.concatenate(rows, axis=0)

    qt[...] = turned(projected[:, 0:128].T) * HEAD**-0.5
    keys[...] = turned(projected[:, 128:256].T)
    values[...] = projected[:, 256:384].T
    gating = projected[:, 384:512]

    for h in range(2):
        at = slice(h * HEAD, (h + 1) * HEAD)
        total = jnp.zeros((HEAD, ROWS), F32)
        for i in range(h * PER_HEAD, (h + 1) * PER_HEAD):
            in_copies[i].wait()
            first = (i % PER_HEAD) * STEP

            def step(s, total):
                k = first + s
                return total + qt[pl.ds(h * HEAD + k, 1), :] * old[h, k]

            total = lax.fori_loop(0, STEP, step, total, unroll=8)
        match = jnp.sum(qt[at, :] * keys[at, :], axis=0, keepdims=True)
        total = decays[first_head + h] * total + match * values[at, :]
        center = total - jnp.mean(total, axis=0, keepdims=True)
        spread = jnp.mean(center * center, axis=0, keepdims=True)
        ret[h * HEAD : (h + 1) * HEAD, :] = center * lax.rsqrt(spread + EPSILON)

    out = (ret[...].T * head_gain[...].astype(F32) * (gating * jax.nn.sigmoid(gating))).astype(BF16)
    wo_copy.wait()
    partial = jnp.dot(out, w_out[...], preferred_element_type=F32)
    shares[...] = partial.reshape(Y, C, SHARE, D)
    core = lax.axis_index("c")
    mine[...] = shares[:, core]
    others[...] = shares[:, 1 - core].astype(BF16)
    at = pl.multiple_of(place(0, False) * SHARE, SHARE)
    own[...] = jnp.concatenate([tokens[j, pl.ds(at, SHARE), :] for j in range(TP)], axis=1)


def retain(blocks, states, wq, wk, wv, wg, wo, mix_gain, head_gain):
    any_space = pl.BlockSpec(memory_space=pl.ANY)
    vmem = pl.BlockSpec(memory_space=pltpu.VMEM)
    return pl.pallas_call(
        retain_kernel,
        out_shape=(
            jax.ShapeDtypeStruct((Y, SHARE, D), F32),
            jax.ShapeDtypeStruct((Y, SHARE, D), BF16),
            jax.ShapeDtypeStruct((SHARE, D), BF16),
            jax.ShapeDtypeStruct((128, ROWS), F32),
            jax.ShapeDtypeStruct((128, ROWS), F32),
        ),
        in_specs=[pl.BlockSpec(memory_space=pltpu.SMEM)]
        + [vmem] * TP + [any_space] * 6 + [vmem] * 4,
        out_specs=(vmem,) * 5,
        scratch_shapes=[
            pltpu.VMEM((TP, ROWS, 256), BF16),
            pltpu.VMEM((D, 512), BF16),
            pltpu.VMEM((128, D), BF16),
            pltpu.VMEM((2, HEAD, HEAD, ROWS), F32),
            pltpu.VMEM((128, ROWS), F32),
            pltpu.VMEM((128, ROWS), F32),
            pltpu.VMEM((Y, C, SHARE, D), F32),
            pltpu.SemaphoreType.DMA((5,)),
            pltpu.SemaphoreType.DMA((CHUNKS,)),
        ],
        compiler_params=pltpu.CompilerParams(vmem_limit_bytes=RETAIN_LIMIT),
        name="retain",
    )(
        in_hbm(DECAYS), in_hbm(blocks[0]), *map(in_vmem, blocks[1:]), *map(in_hbm, (states, wq, wk, wv, wg, wo)),
        *map(in_hbm, (mix_gain.reshape(16, 128), head_gain.reshape(1, 128), COSINE, SINES)),
    )


def update_kernel(decays, keys, values, states, new_states, old, new, in_sems, out_sems):
    first_head = 2 * place(0, False)
    in_copies = [
        pltpu.make_async_copy(part(states, i), part(old, i), in_sems.at[i]) for i in range(CHUNKS)
    ]
    out_copies = [
        pltpu.make_async_copy(part(new, i), part(new_states, i), out_sems.at[i])
        for i in range(CHUNKS)
    ]
    for copy in in_copies:
        copy.start()
    for i in range(CHUNKS):
        h = i // PER_HEAD
        value = values[h * HEAD : (h + 1) * HEAD, :]
        decay = decays[first_head + h]
        in_copies[i].wait()

        def step(s, carry):
            k = (i % PER_HEAD) * STEP + s
            new[h, k] = decay * old[h, k] + keys[pl.ds(h * HEAD + k, 1), :] * value
            return carry

        lax.fori_loop(0, STEP, step, 0, unroll=8)
        out_copies[i].start()
    for copy in out_copies:
        copy.wait()


def update(keys, values, states):
    any_space = pl.BlockSpec(memory_space=pl.ANY)
    vmem = pl.BlockSpec(memory_space=pltpu.VMEM)
    return pl.pallas_call(
        update_kernel,
        out_shape=jax.ShapeDtypeStruct((2, HEAD, HEAD, ROWS), F32),
        in_specs=[pl.BlockSpec(memory_space=pltpu.SMEM), vmem, vmem, any_space],
        out_specs=any_space,
        scratch_shapes=[
            pltpu.VMEM((2, HEAD, HEAD, ROWS), F32),
            pltpu.VMEM((2, HEAD, HEAD, ROWS), F32),
            pltpu.SemaphoreType.DMA((CHUNKS,)),
            pltpu.SemaphoreType.DMA((CHUNKS,)),
        ],
        compiler_params=pltpu.CompilerParams(vmem_limit_bytes=RETAIN_LIMIT),
        name="update",
    )(in_hbm(DECAYS), keys, values, in_hbm(states))


def pair_kernel(mine, others, *outs):
    y = lax.axis_index("y")
    for k in range(Y):
        to = lax.rem(y + k, Y)
        outs[k][...] = (mine[to] + others[to].astype(F32)).astype(outs[k].dtype)


def pair(mine, others):
    vmem = pl.BlockSpec(memory_space=pltpu.VMEM)
    return pl.pallas_call(
        pair_kernel,
        out_shape=[jax.ShapeDtypeStruct((SHARE, D), BF16 if k else F32) for k in range(Y)],
        in_specs=[vmem] * 2,
        out_specs=[vmem] * Y,
        compiler_params=pltpu.CompilerParams(vmem_limit_bytes=8 * 2**20),
        name="pair",
    )(in_vmem(mine), in_vmem(others))


def middle_kernel(own, first, *refs):
    total = first[...]
    for part in refs[:-1]:
        total += part[...].astype(F32)
    middle = (own[...].astype(F32) + total).astype(BF16)
    for z in range(Z):
        refs[-1][z] = middle


def middle_rows(own, parts):
    vmem = pl.BlockSpec(memory_space=pltpu.VMEM)
    return pl.pallas_call(
        middle_kernel,
        out_shape=jax.ShapeDtypeStruct((Z, SHARE, D), BF16),
        in_specs=[vmem] * (Y + 1),
        out_specs=vmem,
        compiler_params=pltpu.CompilerParams(vmem_limit_bytes=8 * 2**20),
        name="middle",
    )(*map(in_vmem, (own, *parts)))


def mixer_kernel(*refs):
    everyone, channel_gain, own_up, own_down = refs[:4]
    ups, downs = refs[4:10], refs[10:16]
    out, rows, up, down, sems = refs[16:]
    row_copy = pltpu.make_async_copy(everyone, rows, sems.at[27])
    row_copy.start()
    up_copies = [pltpu.make_async_copy(own_up, up.at[:, :, pl.ds(0, 256)], sems.at[0])]
    down_copies = [
        pltpu.make_async_copy(
            own_down.at[:, pl.ds(256 * j, 256)], down.at[j, pl.ds(0, 256)], sems.at[1 + j]
        )
        for j in range(8)
    ]
    for p in range(6):
        at = 256 + 128 * p
        for i in range(2):
            up_copies.append(
                pltpu.make_async_copy(
                    ups[p].at[pl.ds(0, 8), :, pl.ds(128 * i, 128)],
                    up.at[pl.ds(8 * i, 8), :, pl.ds(at, 128)],
                    sems.at[9 + 3 * p + i],
                )
            )
        down_copies.append(
            pltpu.make_async_copy(
                downs[p].at[pl.ds(downs[p].shape[0] - 8, 8)],
                down.at[:, pl.ds(at, 128), :],
                sems.at[9 + 3 * p + 2],
            )
        )
    for copy in up_copies + down_copies:
        copy.start()
    row_copy.wait()
    squares = jnp.zeros((ROWS, 256), F32)
    scaled = []
    for j in range(TP):
        wide = rows[:, :, 256 * j : 256 * j + 256].reshape(ROWS, 256).astype(F32)
        squares += wide * wide
        scaled.append((wide * gain_row(channel_gain, j)).astype(BF16))
    second_rms = lax.rsqrt(jnp.sum(squares, axis=1, keepdims=True) / D + EPSILON)
    scaled = jnp.concatenate(scaled, axis=1)
    activated = []
    for n in range(4):
        for copy in up_copies[0:1] if n == 0 else up_copies[4 * n - 3 : 4 * n + 1]:
            copy.wait()
        hidden = second_rms * jnp.dot(
            scaled,
            up[:, :, 256 * n : 256 * n + 256].reshape(D, 256),
            preferred_element_type=F32,
        )
        activated.append(jnp.square(jax.nn.relu(hidden)).astype(BF16))
    activated = jnp.concatenate(activated, axis=1)
    for copy in down_copies:
        copy.wait()
    row = lax.broadcasted_iota(jnp.int32, (ROWS, 1), 0)
    mine = row // SHARE == lax.axis_index("z")
    for j in range(TP):
        part = jnp.dot(activated, down[j], preferred_element_type=F32)
        own = rows[:, :, 256 * j : 256 * j + 256].reshape(ROWS, 256).astype(F32)
        part = part + jnp.where(mine, own, 0.0)
        out[:, j] = part.astype(BF16).reshape(Z, SHARE, 256)


def mixer(rows, channel_gain, own_up, own_down, ups, downs):
    any_space = pl.BlockSpec(memory_space=pl.ANY)
    vmem = pl.BlockSpec(memory_space=pltpu.VMEM)
    return pl.pallas_call(
        mixer_kernel,
        out_shape=pltpu.VMEM((Z, TP, SHARE, 256), BF16),
        in_specs=[any_space, vmem] + [any_space] * 14,
        out_specs=vmem,
        scratch_shapes=[
            pltpu.VMEM((Z, SHARE, D), BF16),
            pltpu.VMEM((16, 128, 1024), BF16),
            pltpu.VMEM((8, 1024, 256), BF16),
            pltpu.SemaphoreType.DMA((28,)),
        ],
        compiler_params=pltpu.CompilerParams(vmem_limit_bytes=MIXER_LIMIT),
        name="mixer",
    )(
        in_hbm(rows), in_hbm(channel_gain.reshape(16, 128)), in_hbm(own_up.reshape(16, 128, 256)),
        in_hbm(own_down), *map(in_hbm, ups), *map(in_hbm, downs),
    )


def shift(count, by):
    return [(i, (i + by) % count) for i in range(count)]


def to_all(array, axes):
    return lax.all_to_all(array, axes, 0, 0, tiled=True)


def local(
    tokens, states, mix_gain, w_query, w_key, w_value, w_gate, head_gain, w_output,
    channel_gain, w_up, w_down,
):
    swap = [(0, 1), (1, 0)]
    blocks = [tokens] + [lax.ppermute(tokens, "y", shift(Y, by)) for by in (1, 2, 3)]
    packed_up, packed_down = pack(w_up, w_down)
    left_up = lax.ppermute(packed_up, "x", shift(X, 1))
    right_down = lax.ppermute(packed_down, "x", shift(X, 3))
    blocks += [lax.ppermute(block, "c", swap) for block in blocks]
    states = states.transpose(1, 2, 3, 0)
    mine, others, own, keys, values = retain(
        blocks, states, w_query, w_key, w_value, w_gate, w_output, mix_gain, head_gain
    )
    others = lax.ppermute(others, "c", swap)
    right_up = lax.ppermute(packed_up, "x", shift(X, 3))
    left_down = lax.ppermute(packed_down, "x", shift(X, 1))
    parts = pair(mine, others)
    parts = [parts[0]] + [lax.ppermute(parts[k], "y", shift(Y, k)) for k in (1, 2, 3)]
    middle = middle_rows(own, parts)
    everyone = to_all(middle, "z")
    far_up = lax.ppermute(left_up, "x", shift(X, 1))
    far_down = lax.ppermute(right_down, "x", shift(X, 3))
    new_states = update(keys, values, states)
    near_other = [lax.ppermute(w, "c", swap) for w in (left_up, right_down)]
    near_other += [lax.ppermute(w, "c", swap) for w in (right_up, left_down)]
    far_up, far_down, *near_other = lax.optimization_barrier((far_up, far_down, *near_other))
    far_other = [lax.ppermute(w, "c", swap) for w in (far_up, far_down)]
    down = mixer(
        everyone, channel_gain, w_up, w_down,
        (left_up, near_other[0], right_up, near_other[2], far_up, far_other[0]),
        (left_down, near_other[3], right_down, near_other[1], far_down, far_other[1]),
    )
    down = to_all(down.reshape(Z * TP, SHARE, 256), ("z", "y", "c"))
    layer_out = jnp.sum(down.reshape(Z, ROWS, 256).astype(F32), axis=0).astype(BF16)
    return (layer_out, new_states.transpose(3, 0, 1, 2))


def solution(mesh):
    torus = Mesh(mesh.devices.reshape(Z, X, Y, C), ("z", "x", "y", "c"))
    kv, tp = ("z", "x"), ("y", "c")
    in_specs = (
        P(kv, tp), P(kv, tp, None, None), P(), P(None, tp), P(None, tp), P(None, tp), P(None, tp),
        P(tp), P(tp, None), P(), P(None, kv), P(kv, None),
    )
    out_specs = (P(kv, tp), P(kv, tp, None, None))
    return jax.shard_map(local, mesh=torus, in_specs=in_specs, out_specs=out_specs, check_vma=False)
```

```python
import jax
import jax.numpy as jnp
import numpy as np
from jax import lax
from jax.experimental import pallas as pl
from jax.experimental.pallas import tpu as pltpu
from jax.sharding import Mesh
from jax.sharding import PartitionSpec as P


HEADS = 16
HEAD = 64
POS = 16384
D = 2048
EPSILON = 1e-06
ROTARY_BASE = 10000.0
ROWS = 128
Z, X, Y, C = 8, 4, 4, 2
TP = Y * C
SHARE = ROWS // TP
RETAIN_LIMIT = 14 * 2**20
MIXER_LIMIT = 14 * 2**20
F32 = jnp.float32
BF16 = jnp.bfloat16


def in_hbm(array):
    return pltpu.with_memory_space_constraint(array, pltpu.HBM)


def in_vmem(array):
    return pltpu.with_memory_space_constraint(array, pltpu.VMEM)


def copy_all(copies):
    for copy in copies:
        copy.start()
    for copy in copies:
        copy.wait()


def pack_kernel(up, down, packed_up, packed_down, sems):
    at = pl.multiple_of(lax.axis_index("c") * 128, 128)
    copies = [
        pltpu.make_async_copy(
            up.at[pl.ds(8 * i, 8), :, pl.ds(at, 128)],
            packed_up.at[:, :, pl.ds(128 * i, 128)],
            sems.at[i],
        )
        for i in range(2)
    ]
    copies += [
        pltpu.make_async_copy(
            down.at[pl.ds(at, 128), pl.ds(256 * j, 256)], packed_down.at[j], sems.at[2 + j]
        )
        for j in range(8)
    ]
    copy_all(copies)


def pack(w_up, w_down):
    return pl.pallas_call(
        pack_kernel,
        out_shape=[jax.ShapeDtypeStruct((8, 128, 256), BF16)] * 2,
        in_specs=[pl.BlockSpec(memory_space=pl.ANY)] * 2,
        out_specs=[pl.BlockSpec(memory_space=pltpu.VMEM)] * 2,
        scratch_shapes=[pltpu.SemaphoreType.DMA((10,))],
        compiler_params=pltpu.CompilerParams(vmem_limit_bytes=8 * 2**20),
        name="pack",
    )(in_hbm(w_up.reshape(16, 128, 256)), in_hbm(w_down))


CHUNKS = 8
PER_HEAD = CHUNKS // 2
STEP = HEAD // PER_HEAD
ANGLES = POS * ROTARY_BASE ** (-np.arange(HEAD // 2) / (HEAD // 2))
COSINE = np.broadcast_to(np.cos(ANGLES)[:, None], (HEAD // 2, ROWS)).astype(np.float32)
SINES = np.broadcast_to(np.sin(ANGLES)[:, None], (HEAD // 2, ROWS)).astype(np.float32)
DECAYS = (1.0 - 2.0 ** (-1.0 - 11.0 * np.arange(HEADS) / (HEADS - 1))).astype(np.float32)


def gain_row(gain, j):
    wide = gain[...].astype(F32)
    return jnp.concatenate([wide[2 * j : 2 * j + 1], wide[2 * j + 1 : 2 * j + 2]], axis=1)


def place(k, other):
    y, c = lax.axis_index("y"), lax.axis_index("c")
    return 2 * lax.rem(y + (Y - k), Y) + (1 - c if other else c)


def part(ref, i):
    return ref.at[i // PER_HEAD, pl.ds((i % PER_HEAD) * STEP, STEP)]


def retain_kernel(decays, *refs):
    blocks = refs[:TP]
    states, wq, wk, wv, wg, wo, mix_gain, head_gain, cosine, sines = refs[TP : TP + 10]
    mine, others, own, keys, values = refs[TP + 10 : TP + 15]
    tokens, weights, w_out, old, qt, ret, shares = refs[TP + 15 : TP + 22]
    w_sems, in_sems = refs[TP + 22 :]

    first_head = 2 * (lax.axis_index("y") * C + lax.axis_index("c"))
    w_copies = [
        pltpu.make_async_copy(w, weights.at[:, pl.ds(128 * i, 128)], w_sems.at[i])
        for i, w in enumerate((wq, wk, wv, wg))
    ]
    wo_copy = pltpu.make_async_copy(wo, w_out, w_sems.at[4])
    in_copies = [
        pltpu.make_async_copy(part(states, i), part(old, i), in_sems.at[i]) for i in range(CHUNKS)
    ]
    for copy in w_copies + in_copies + [wo_copy]:
        copy.start()

    squares = jnp.zeros((ROWS, 256), F32)
    for i in range(TP):
        block = blocks[i][...]
        tokens[place(i % Y, i >= Y)] = block
        block = block.astype(F32)
        squares += block * block
    inverse_rms = lax.rsqrt(jnp.sum(squares, axis=1, keepdims=True) / D + EPSILON)
    normed = jnp.concatenate(
        [
            (tokens[j].astype(F32) * inverse_rms * gain_row(mix_gain, j)).astype(BF16)
            for j in range(TP)
        ],
        axis=1,
    )
    for copy in w_copies:
        copy.wait()
    projected = jnp.dot(normed, weights[...], preferred_element_type=F32)
    half = HEAD // 2

    def turned(flat):
        rows = []
        for h in range(2):
            a = flat[h * HEAD : h * HEAD + half]
            b = flat[h * HEAD + half : (h + 1) * HEAD]
            rows += [a * cosine[...] - b * sines[...], a * sines[...] + b * cosine[...]]
        return jnp.concatenate(rows, axis=0)

    qt[...] = turned(projected[:, 0:128].T) * HEAD**-0.5
    keys[...] = turned(projected[:, 128:256].T)
    values[...] = projected[:, 256:384].T
    gating = projected[:, 384:512]

    for h in range(2):
        at = slice(h * HEAD, (h + 1) * HEAD)
        total = jnp.zeros((HEAD, ROWS), F32)
        for i in range(h * PER_HEAD, (h + 1) * PER_HEAD):
            in_copies[i].wait()
            first = (i % PER_HEAD) * STEP

            def step(s, total):
                k = first + s
                return total + qt[pl.ds(h * HEAD + k, 1), :] * old[h, k]

            total = lax.fori_loop(0, STEP, step, total, unroll=8)
        match = jnp.sum(qt[at, :] * keys[at, :], axis=0, keepdims=True)
        total = decays[first_head + h] * total + match * values[at, :]
        center = total - jnp.mean(total, axis=0, keepdims=True)
        spread = jnp.mean(center * center, axis=0, keepdims=True)
        ret[h * HEAD : (h + 1) * HEAD, :] = center * lax.rsqrt(spread + EPSILON)

    out = (ret[...].T * head_gain[...].astype(F32) * (gating * jax.nn.sigmoid(gating))).astype(BF16)
    wo_copy.wait()
    partial = jnp.dot(out, w_out[...], preferred_element_type=F32)
    shares[...] = partial.reshape(Y, C, SHARE, D)
    core = lax.axis_index("c")
    mine[...] = shares[:, core]
    others[...] = shares[:, 1 - core].astype(BF16)
    at = pl.multiple_of(place(0, False) * SHARE, SHARE)
    own[...] = jnp.concatenate([tokens[j, pl.ds(at, SHARE), :] for j in range(TP)], axis=1)


def retain(blocks, states, wq, wk, wv, wg, wo, mix_gain, head_gain):
    any_space = pl.BlockSpec(memory_space=pl.ANY)
    vmem = pl.BlockSpec(memory_space=pltpu.VMEM)
    return pl.pallas_call(
        retain_kernel,
        out_shape=(
            jax.ShapeDtypeStruct((Y, SHARE, D), F32),
            jax.ShapeDtypeStruct((Y, SHARE, D), BF16),
            jax.ShapeDtypeStruct((SHARE, D), BF16),
            jax.ShapeDtypeStruct((128, ROWS), F32),
            jax.ShapeDtypeStruct((128, ROWS), F32),
        ),
        in_specs=[pl.BlockSpec(memory_space=pltpu.SMEM)]
        + [vmem] * TP + [any_space] * 6 + [vmem] * 4,
        out_specs=(vmem,) * 5,
        scratch_shapes=[
            pltpu.VMEM((TP, ROWS, 256), BF16),
            pltpu.VMEM((D, 512), BF16),
            pltpu.VMEM((128, D), BF16),
            pltpu.VMEM((2, HEAD, HEAD, ROWS), F32),
            pltpu.VMEM((128, ROWS), F32),
            pltpu.VMEM((128, ROWS), F32),
            pltpu.VMEM((Y, C, SHARE, D), F32),
            pltpu.SemaphoreType.DMA((5,)),
            pltpu.SemaphoreType.DMA((CHUNKS,)),
        ],
        compiler_params=pltpu.CompilerParams(vmem_limit_bytes=RETAIN_LIMIT),
        name="retain",
    )(
        in_hbm(DECAYS), in_hbm(blocks[0]), *map(in_vmem, blocks[1:]), *map(in_hbm, (states, wq, wk, wv, wg, wo)),
        *map(in_hbm, (mix_gain.reshape(16, 128), head_gain.reshape(1, 128), COSINE, SINES)),
    )


def update_kernel(decays, keys, values, states, new_states, old, new, in_sems, out_sems):
    first_head = 2 * place(0, False)
    in_copies = [
        pltpu.make_async_copy(part(states, i), part(old, i), in_sems.at[i]) for i in range(CHUNKS)
    ]
    out_copies = [
        pltpu.make_async_copy(part(new, i), part(new_states, i), out_sems.at[i])
        for i in range(CHUNKS)
    ]
    for copy in in_copies:
        copy.start()
    for i in range(CHUNKS):
        h = i // PER_HEAD
        value = values[h * HEAD : (h + 1) * HEAD, :]
        decay = decays[first_head + h]
        in_copies[i].wait()

        def step(s, carry):
            k = (i % PER_HEAD) * STEP + s
            new[h, k] = decay * old[h, k] + keys[pl.ds(h * HEAD + k, 1), :] * value
            return carry

        lax.fori_loop(0, STEP, step, 0, unroll=8)
        out_copies[i].start()
    for copy in out_copies:
        copy.wait()


def update(keys, values, states):
    any_space = pl.BlockSpec(memory_space=pl.ANY)
    vmem = pl.BlockSpec(memory_space=pltpu.VMEM)
    return pl.pallas_call(
        update_kernel,
        out_shape=jax.ShapeDtypeStruct((2, HEAD, HEAD, ROWS), F32),
        in_specs=[pl.BlockSpec(memory_space=pltpu.SMEM), vmem, vmem, any_space],
        out_specs=any_space,
        scratch_shapes=[
            pltpu.VMEM((2, HEAD, HEAD, ROWS), F32),
            pltpu.VMEM((2, HEAD, HEAD, ROWS), F32),
            pltpu.SemaphoreType.DMA((CHUNKS,)),
            pltpu.SemaphoreType.DMA((CHUNKS,)),
        ],
        compiler_params=pltpu.CompilerParams(vmem_limit_bytes=RETAIN_LIMIT),
        name="update",
    )(in_hbm(DECAYS), keys, values, in_hbm(states))


def pair_kernel(mine, others, *outs):
    y = lax.axis_index("y")
    for k in range(Y):
        to = lax.rem(y + k, Y)
        outs[k][...] = (mine[to] + others[to].astype(F32)).astype(outs[k].dtype)


def pair(mine, others):
    vmem = pl.BlockSpec(memory_space=pltpu.VMEM)
    return pl.pallas_call(
        pair_kernel,
        out_shape=[jax.ShapeDtypeStruct((SHARE, D), BF16 if k else F32) for k in range(Y)],
        in_specs=[vmem] * 2,
        out_specs=[vmem] * Y,
        compiler_params=pltpu.CompilerParams(vmem_limit_bytes=8 * 2**20),
        name="pair",
    )(in_vmem(mine), in_vmem(others))


def middle_kernel(own, first, *refs):
    total = first[...]
    for part in refs[:-1]:
        total += part[...].astype(F32)
    middle = (own[...].astype(F32) + total).astype(BF16)
    for z in range(Z):
        refs[-1][z] = middle


def middle_rows(own, parts):
    vmem = pl.BlockSpec(memory_space=pltpu.VMEM)
    return pl.pallas_call(
        middle_kernel,
        out_shape=jax.ShapeDtypeStruct((Z, SHARE, D), BF16),
        in_specs=[vmem] * (Y + 1),
        out_specs=vmem,
        compiler_params=pltpu.CompilerParams(vmem_limit_bytes=8 * 2**20),
        name="middle",
    )(*map(in_vmem, (own, *parts)))


def piece_copies(ups, downs, up, down, at, sems):
    up_copies, down_copies = [], []
    for p in range(len(ups)):
        to = at + 128 * p
        for i in range(2):
            up_copies.append(
                pltpu.make_async_copy(
                    ups[p].at[:, :, pl.ds(128 * i, 128)],
                    up.at[pl.ds(8 * i, 8), :, pl.ds(to, 128)],
                    sems.at[3 * p + i],
                )
            )
        down_copies.append(
            pltpu.make_async_copy(downs[p], down.at[:, pl.ds(to, 128), :], sems.at[3 * p + 2])
        )
    return up_copies, down_copies


def hidden_units(scaled, up, n, second_rms):
    weight = up[:, :, 256 * n : 256 * n + 256].reshape(D, 256)
    hidden = second_rms * jnp.dot(scaled, weight, preferred_element_type=F32)
    return jnp.square(jax.nn.relu(hidden)).astype(BF16)


def mixer_kernel(*refs):
    everyone, channel_gain, own_up, own_down = refs[:4]
    ups, downs = refs[4:8], refs[8:12]
    base, scaled_out, rms_out, rows, up, down, own_sems, sems = refs[12:]
    row_copy = pltpu.make_async_copy(everyone, rows, own_sems.at[0])
    row_copy.start()
    up_copies, down_copies = piece_copies(ups, downs, up, down, 256, sems)
    up_copies.insert(
        0, pltpu.make_async_copy(own_up, up.at[:, :, pl.ds(0, 256)], own_sems.at[1])
    )
    down_copies += [
        pltpu.make_async_copy(
            own_down.at[:, pl.ds(256 * j, 256)], down.at[j, pl.ds(0, 256)], own_sems.at[2 + j]
        )
        for j in range(8)
    ]
    for copy in up_copies + down_copies:
        copy.start()
    row_copy.wait()
    squares = jnp.zeros((ROWS, 256), F32)
    scaled = []
    for j in range(TP):
        wide = rows[:, :, 256 * j : 256 * j + 256].reshape(ROWS, 256).astype(F32)
        squares += wide * wide
        scaled.append((wide * gain_row(channel_gain, j)).astype(BF16))
    second_rms = lax.rsqrt(jnp.sum(squares, axis=1, keepdims=True) / D + EPSILON)
    rms_out[...] = jnp.broadcast_to(second_rms, (ROWS, 128))
    scaled = jnp.concatenate(scaled, axis=1)
    scaled_out[...] = scaled
    activated = []
    for n in range(3):
        for copy in up_copies[0:1] if n == 0 else up_copies[4 * n - 3 : 4 * n + 1]:
            copy.wait()
        activated.append(hidden_units(scaled, up, n, second_rms))
    activated = jnp.concatenate(activated, axis=1)
    for copy in down_copies:
        copy.wait()
    row = lax.broadcasted_iota(jnp.int32, (ROWS, 1), 0)
    mine = row // SHARE == lax.axis_index("z")
    for j in range(TP):
        part = jnp.dot(activated, down[j], preferred_element_type=F32)
        own = rows[:, :, 256 * j : 256 * j + 256].reshape(ROWS, 256).astype(F32)
        base[j] = part + jnp.where(mine, own, 0.0)


def mixer(rows, channel_gain, own_up, own_down, ups, downs):
    any_space = pl.BlockSpec(memory_space=pl.ANY)
    vmem = pl.BlockSpec(memory_space=pltpu.VMEM)
    return pl.pallas_call(
        mixer_kernel,
        out_shape=(
            jax.ShapeDtypeStruct((TP, ROWS, 256), F32),
            jax.ShapeDtypeStruct((ROWS, D), BF16),
            jax.ShapeDtypeStruct((ROWS, 128), F32),
        ),
        in_specs=[any_space, vmem] + [any_space] * 10,
        out_specs=(vmem,) * 3,
        scratch_shapes=[
            pltpu.VMEM((Z, SHARE, D), BF16),
            pltpu.VMEM((16, 128, 768), BF16),
            pltpu.VMEM((8, 768, 256), BF16),
            pltpu.SemaphoreType.DMA((10,)),
            pltpu.SemaphoreType.DMA((12,)),
        ],
        compiler_params=pltpu.CompilerParams(vmem_limit_bytes=MIXER_LIMIT),
        name="mixer",
    )(
        rows, in_hbm(channel_gain.reshape(16, 128)), in_hbm(own_up.reshape(16, 128, 256)),
        in_hbm(own_down), *ups, *downs,
    )


def finish_kernel(base, scaled, rms, *refs):
    ups, downs = refs[:2], refs[2:4]
    out, up, down, sems = refs[4:]
    up_copies, down_copies = piece_copies(ups, downs, up, down, 0, sems)
    for copy in up_copies + down_copies:
        copy.start()
    for copy in up_copies:
        copy.wait()
    activated = hidden_units(scaled[...], up, 0, rms[:, 0:1])
    for copy in down_copies:
        copy.wait()
    for j in range(TP):
        part = base[j] + jnp.dot(activated, down[j], preferred_element_type=F32)
        out[:, j] = part.astype(BF16).reshape(Z, SHARE, 256)


def finish(base, scaled, rms, ups, downs):
    any_space = pl.BlockSpec(memory_space=pl.ANY)
    vmem = pl.BlockSpec(memory_space=pltpu.VMEM)
    return pl.pallas_call(
        finish_kernel,
        out_shape=jax.ShapeDtypeStruct((Z, TP, SHARE, 256), BF16),
        in_specs=[vmem] * 3 + [any_space] * 4,
        out_specs=vmem,
        scratch_shapes=[
            pltpu.VMEM((16, 128, 256), BF16),
            pltpu.VMEM((8, 256, 256), BF16),
            pltpu.SemaphoreType.DMA((6,)),
        ],
        compiler_params=pltpu.CompilerParams(vmem_limit_bytes=MIXER_LIMIT),
        name="finish",
    )(in_vmem(base), in_vmem(scaled), in_vmem(rms), *ups, *downs)


def shift(count, by):
    return [(i, (i + by) % count) for i in range(count)]


def to_all(array, axes):
    return lax.all_to_all(array, axes, 0, 0, tiled=True)


def local(
    tokens, states, mix_gain, w_query, w_key, w_value, w_gate, head_gain, w_output,
    channel_gain, w_up, w_down,
):
    swap = [(0, 1), (1, 0)]
    blocks = [tokens] + [lax.ppermute(tokens, "y", shift(Y, by)) for by in (1, 2, 3)]
    packed_up, packed_down = pack(w_up, w_down)
    left_up = lax.ppermute(packed_up, "x", shift(X, 1))
    right_down = lax.ppermute(packed_down, "x", shift(X, 3))
    blocks += [lax.ppermute(block, "c", swap) for block in blocks]
    states = states.transpose(1, 2, 3, 0)
    mine, others, own, keys, values = retain(
        blocks, states, w_query, w_key, w_value, w_gate, w_output, mix_gain, head_gain
    )
    others = lax.ppermute(others, "c", swap)
    right_up = lax.ppermute(packed_up, "x", shift(X, 3))
    left_down = lax.ppermute(packed_down, "x", shift(X, 1))
    parts = pair(mine, others)
    parts = [parts[0]] + [lax.ppermute(parts[k], "y", shift(Y, k)) for k in (1, 2, 3)]
    middle = middle_rows(own, parts)
    everyone = to_all(middle, "z")
    far_up = lax.ppermute(left_up, "x", shift(X, 1))
    far_down = lax.ppermute(right_down, "x", shift(X, 3))
    new_states = update(keys, values, states)
    near_other = [lax.ppermute(w, "c", swap) for w in (left_up, right_down)]
    near_other += [lax.ppermute(w, "c", swap) for w in (right_up, left_down)]
    far_up, far_down, *near_other = lax.optimization_barrier((far_up, far_down, *near_other))
    far_other = [lax.ppermute(w, "c", swap) for w in (far_up, far_down)]
    near_other = [in_hbm(w) for w in near_other]
    right_up, left_down = in_hbm(right_up), in_hbm(left_down)
    base, scaled, rms = mixer(
        everyone, channel_gain, w_up, w_down,
        (left_up, near_other[0], right_up, near_other[2]),
        (left_down, near_other[3], right_down, near_other[1]),
    )
    far_up, far_down = in_hbm(far_up), in_hbm(far_down)
    down = finish(base, scaled, rms, (far_up, far_other[0]), (far_down, far_other[1]))
    down = to_all(down.reshape(Z * TP, SHARE, 256), ("z", "y", "c"))
    layer_out = jnp.sum(down.reshape(Z, ROWS, 256).astype(F32), axis=0).astype(BF16)
    return (layer_out, new_states.transpose(3, 0, 1, 2))


def solution(mesh):
    torus = Mesh(mesh.devices.reshape(Z, X, Y, C), ("z", "x", "y", "c"))
    kv, tp = ("z", "x"), ("y", "c")
    in_specs = (
        P(kv, tp), P(kv, tp, None, None), P(), P(None, tp), P(None, tp), P(None, tp), P(None, tp),
        P(tp), P(tp, None), P(), P(None, kv), P(kv, None),
    )
    out_specs = (P(kv, tp), P(kv, tp, None, None))
    return jax.shard_map(local, mesh=torus, in_specs=in_specs, out_specs=out_specs, check_vma=False)
```

```python
import jax
import jax.numpy as jnp
import numpy as np
from jax import lax
from jax.experimental import pallas as pl
from jax.experimental.pallas import tpu as pltpu
from jax.sharding import Mesh
from jax.sharding import PartitionSpec as P


HEADS = 16
HEAD = 64
POS = 16384
D = 2048
EPSILON = 1e-06
ROTARY_BASE = 10000.0
ROWS = 128
Z, X, Y, C = 8, 4, 4, 2
TP = Y * C
SHARE = ROWS // TP
RETAIN_LIMIT = 14 * 2**20
MIXER_LIMIT = 14 * 2**20
F32 = jnp.float32
BF16 = jnp.bfloat16


def in_hbm(array):
    return pltpu.with_memory_space_constraint(array, pltpu.HBM)


def in_vmem(array):
    return pltpu.with_memory_space_constraint(array, pltpu.VMEM)


def copy_all(copies):
    for copy in copies:
        copy.start()
    for copy in copies:
        copy.wait()


def pack_kernel(up, down, packed_up, packed_down, sems):
    at = pl.multiple_of(lax.axis_index("c") * 128, 128)
    copies = [
        pltpu.make_async_copy(
            up.at[pl.ds(8 * i, 8), :, pl.ds(at, 128)],
            packed_up.at[:, :, pl.ds(128 * i, 128)],
            sems.at[i],
        )
        for i in range(2)
    ]
    copies += [
        pltpu.make_async_copy(
            down.at[pl.ds(at, 128), pl.ds(256 * j, 256)], packed_down.at[j], sems.at[2 + j]
        )
        for j in range(8)
    ]
    copy_all(copies)


def pack(w_up, w_down):
    return pl.pallas_call(
        pack_kernel,
        out_shape=[jax.ShapeDtypeStruct((8, 128, 256), BF16)] * 2,
        in_specs=[pl.BlockSpec(memory_space=pl.ANY)] * 2,
        out_specs=[pl.BlockSpec(memory_space=pltpu.VMEM)] * 2,
        scratch_shapes=[pltpu.SemaphoreType.DMA((10,))],
        compiler_params=pltpu.CompilerParams(vmem_limit_bytes=8 * 2**20),
        name="pack",
    )(in_hbm(w_up.reshape(16, 128, 256)), in_hbm(w_down))


CHUNKS = 8
PER_HEAD = CHUNKS // 2
STEP = HEAD // PER_HEAD
ANGLES = POS * ROTARY_BASE ** (-np.arange(HEAD // 2) / (HEAD // 2))
COSINE = np.broadcast_to(np.cos(ANGLES)[:, None], (HEAD // 2, ROWS)).astype(np.float32)
SINES = np.broadcast_to(np.sin(ANGLES)[:, None], (HEAD // 2, ROWS)).astype(np.float32)
DECAYS = (1.0 - 2.0 ** (-1.0 - 11.0 * np.arange(HEADS) / (HEADS - 1))).astype(np.float32)


def gain_row(gain, j):
    wide = gain[...].astype(F32)
    return jnp.concatenate([wide[2 * j : 2 * j + 1], wide[2 * j + 1 : 2 * j + 2]], axis=1)


def place(k, other):
    y, c = lax.axis_index("y"), lax.axis_index("c")
    return 2 * lax.rem(y + (Y - k), Y) + (1 - c if other else c)


def part(ref, i):
    return ref.at[i // PER_HEAD, pl.ds((i % PER_HEAD) * STEP, STEP)]


def retain_kernel(decays, *refs):
    blocks = refs[:TP]
    states, wq, wk, wv, wg, wo, mix_gain, head_gain, cosine, sines = refs[TP : TP + 10]
    mine, others, own, keys, values = refs[TP + 10 : TP + 15]
    tokens, weights, w_out, old, qt, ret, shares = refs[TP + 15 : TP + 22]
    w_sems, in_sems = refs[TP + 22 :]

    first_head = 2 * (lax.axis_index("y") * C + lax.axis_index("c"))
    w_copies = [
        pltpu.make_async_copy(w, weights.at[:, pl.ds(128 * i, 128)], w_sems.at[i])
        for i, w in enumerate((wq, wk, wv, wg))
    ]
    wo_copy = pltpu.make_async_copy(wo, w_out, w_sems.at[4])
    in_copies = [
        pltpu.make_async_copy(part(states, i), part(old, i), in_sems.at[i]) for i in range(CHUNKS)
    ]
    for copy in w_copies + in_copies + [wo_copy]:
        copy.start()

    squares = jnp.zeros((ROWS, 256), F32)
    for i in range(TP):
        block = blocks[i][...]
        tokens[place(i % Y, i >= Y)] = block
        block = block.astype(F32)
        squares += block * block
    inverse_rms = lax.rsqrt(jnp.sum(squares, axis=1, keepdims=True) / D + EPSILON)
    normed = jnp.concatenate(
        [
            (tokens[j].astype(F32) * inverse_rms * gain_row(mix_gain, j)).astype(BF16)
            for j in range(TP)
        ],
        axis=1,
    )
    for copy in w_copies:
        copy.wait()
    projected = jnp.dot(normed, weights[...], preferred_element_type=F32)
    half = HEAD // 2

    def turned(flat):
        rows = []
        for h in range(2):
            a = flat[h * HEAD : h * HEAD + half]
            b = flat[h * HEAD + half : (h + 1) * HEAD]
            rows += [a * cosine[...] - b * sines[...], a * sines[...] + b * cosine[...]]
        return jnp.concatenate(rows, axis=0)

    qt[...] = turned(projected[:, 0:128].T) * HEAD**-0.5
    keys[...] = turned(projected[:, 128:256].T)
    values[...] = projected[:, 256:384].T
    gating = projected[:, 384:512]

    for h in range(2):
        at = slice(h * HEAD, (h + 1) * HEAD)
        total = jnp.zeros((HEAD, ROWS), F32)
        for i in range(h * PER_HEAD, (h + 1) * PER_HEAD):
            in_copies[i].wait()
            first = (i % PER_HEAD) * STEP

            def step(s, total):
                k = first + s
                return total + qt[pl.ds(h * HEAD + k, 1), :] * old[h, k]

            total = lax.fori_loop(0, STEP, step, total, unroll=8)
        match = jnp.sum(qt[at, :] * keys[at, :], axis=0, keepdims=True)
        total = decays[first_head + h] * total + match * values[at, :]
        center = total - jnp.mean(total, axis=0, keepdims=True)
        spread = jnp.mean(center * center, axis=0, keepdims=True)
        ret[h * HEAD : (h + 1) * HEAD, :] = center * lax.rsqrt(spread + EPSILON)

    out = (ret[...].T * head_gain[...].astype(F32) * (gating * jax.nn.sigmoid(gating))).astype(BF16)
    wo_copy.wait()
    partial = jnp.dot(out, w_out[...], preferred_element_type=F32)
    shares[...] = partial.reshape(Y, C, SHARE, D)
    core = lax.axis_index("c")
    mine[...] = shares[:, core]
    others[...] = shares[:, 1 - core].astype(BF16)
    at = pl.multiple_of(place(0, False) * SHARE, SHARE)
    own[...] = jnp.concatenate([tokens[j, pl.ds(at, SHARE), :] for j in range(TP)], axis=1)


def retain(blocks, states, wq, wk, wv, wg, wo, mix_gain, head_gain):
    any_space = pl.BlockSpec(memory_space=pl.ANY)
    vmem = pl.BlockSpec(memory_space=pltpu.VMEM)
    return pl.pallas_call(
        retain_kernel,
        out_shape=(
            jax.ShapeDtypeStruct((Y, SHARE, D), F32),
            jax.ShapeDtypeStruct((Y, SHARE, D), BF16),
            jax.ShapeDtypeStruct((SHARE, D), BF16),
            jax.ShapeDtypeStruct((128, ROWS), F32),
            jax.ShapeDtypeStruct((128, ROWS), F32),
        ),
        in_specs=[pl.BlockSpec(memory_space=pltpu.SMEM)]
        + [vmem] * TP + [any_space] * 6 + [vmem] * 4,
        out_specs=(vmem,) * 5,
        scratch_shapes=[
            pltpu.VMEM((TP, ROWS, 256), BF16),
            pltpu.VMEM((D, 512), BF16),
            pltpu.VMEM((128, D), BF16),
            pltpu.VMEM((2, HEAD, HEAD, ROWS), F32),
            pltpu.VMEM((128, ROWS), F32),
            pltpu.VMEM((128, ROWS), F32),
            pltpu.VMEM((Y, C, SHARE, D), F32),
            pltpu.SemaphoreType.DMA((5,)),
            pltpu.SemaphoreType.DMA((CHUNKS,)),
        ],
        compiler_params=pltpu.CompilerParams(vmem_limit_bytes=RETAIN_LIMIT),
        name="retain",
    )(
        in_hbm(DECAYS), in_hbm(blocks[0]), *map(in_vmem, blocks[1:]), *map(in_hbm, (states, wq, wk, wv, wg, wo)),
        *map(in_hbm, (mix_gain.reshape(16, 128), head_gain.reshape(1, 128), COSINE, SINES)),
    )


def update_kernel(decays, keys, values, states, new_states, old, new, in_sems, out_sems):
    first_head = 2 * place(0, False)
    in_copies = [
        pltpu.make_async_copy(part(states, i), part(old, i), in_sems.at[i]) for i in range(CHUNKS)
    ]
    out_copies = [
        pltpu.make_async_copy(part(new, i), part(new_states, i), out_sems.at[i])
        for i in range(CHUNKS)
    ]
    for copy in in_copies:
        copy.start()
    for i in range(CHUNKS):
        h = i // PER_HEAD
        value = values[h * HEAD : (h + 1) * HEAD, :]
        decay = decays[first_head + h]
        in_copies[i].wait()

        def step(s, carry):
            k = (i % PER_HEAD) * STEP + s
            new[h, k] = decay * old[h, k] + keys[pl.ds(h * HEAD + k, 1), :] * value
            return carry

        lax.fori_loop(0, STEP, step, 0, unroll=8)
        out_copies[i].start()
    for copy in out_copies:
        copy.wait()


def update(keys, values, states):
    any_space = pl.BlockSpec(memory_space=pl.ANY)
    vmem = pl.BlockSpec(memory_space=pltpu.VMEM)
    return pl.pallas_call(
        update_kernel,
        out_shape=jax.ShapeDtypeStruct((2, HEAD, HEAD, ROWS), F32),
        in_specs=[pl.BlockSpec(memory_space=pltpu.SMEM), vmem, vmem, any_space],
        out_specs=any_space,
        scratch_shapes=[
            pltpu.VMEM((2, HEAD, HEAD, ROWS), F32),
            pltpu.VMEM((2, HEAD, HEAD, ROWS), F32),
            pltpu.SemaphoreType.DMA((CHUNKS,)),
            pltpu.SemaphoreType.DMA((CHUNKS,)),
        ],
        compiler_params=pltpu.CompilerParams(vmem_limit_bytes=RETAIN_LIMIT),
        name="update",
    )(in_hbm(DECAYS), keys, values, in_hbm(states))


def pair_kernel(mine, others, *outs):
    y = lax.axis_index("y")
    for k in range(Y):
        to = lax.rem(y + k, Y)
        outs[k][...] = (mine[to] + others[to].astype(F32)).astype(outs[k].dtype)


def pair(mine, others):
    vmem = pl.BlockSpec(memory_space=pltpu.VMEM)
    return pl.pallas_call(
        pair_kernel,
        out_shape=[jax.ShapeDtypeStruct((SHARE, D), BF16 if k else F32) for k in range(Y)],
        in_specs=[vmem] * 2,
        out_specs=[vmem] * Y,
        compiler_params=pltpu.CompilerParams(vmem_limit_bytes=8 * 2**20),
        name="pair",
    )(in_vmem(mine), in_vmem(others))


def middle_kernel(own, first, *refs):
    total = first[...]
    for part in refs[:-1]:
        total += part[...].astype(F32)
    middle = (own[...].astype(F32) + total).astype(BF16)
    for z in range(Z):
        refs[-1][z] = middle


def middle_rows(own, parts):
    vmem = pl.BlockSpec(memory_space=pltpu.VMEM)
    return pl.pallas_call(
        middle_kernel,
        out_shape=jax.ShapeDtypeStruct((Z, SHARE, D), BF16),
        in_specs=[vmem] * (Y + 1),
        out_specs=vmem,
        compiler_params=pltpu.CompilerParams(vmem_limit_bytes=8 * 2**20),
        name="middle",
    )(*map(in_vmem, (own, *parts)))


def mixer_kernel(*refs):
    everyone, channel_gain, own_up, own_down = refs[:4]
    ups, downs = refs[4:10], refs[10:16]
    out, rows, up, down, sems = refs[16:]
    row_copy = pltpu.make_async_copy(everyone, rows, sems.at[27])
    row_copy.start()
    up_copies = [pltpu.make_async_copy(own_up, up.at[:, :, pl.ds(0, 256)], sems.at[0])]
    down_copies = [
        pltpu.make_async_copy(
            own_down.at[:, pl.ds(256 * j, 256)], down.at[j, pl.ds(0, 256)], sems.at[1 + j]
        )
        for j in range(8)
    ]
    for p in range(6):
        at = 256 + 128 * p
        for i in range(2):
            up_copies.append(
                pltpu.make_async_copy(
                    ups[p].at[pl.ds(0, 8), :, pl.ds(128 * i, 128)],
                    up.at[pl.ds(8 * i, 8), :, pl.ds(at, 128)],
                    sems.at[9 + 3 * p + i],
                )
            )
        down_copies.append(
            pltpu.make_async_copy(
                downs[p].at[pl.ds(downs[p].shape[0] - 8, 8)],
                down.at[:, pl.ds(at, 128), :],
                sems.at[9 + 3 * p + 2],
            )
        )
    for copy in up_copies + down_copies:
        copy.start()
    row_copy.wait()
    squares = jnp.zeros((ROWS, 256), F32)
    scaled = []
    for j in range(TP):
        wide = rows[:, :, 256 * j : 256 * j + 256].reshape(ROWS, 256).astype(F32)
        squares += wide * wide
        scaled.append((wide * gain_row(channel_gain, j)).astype(BF16))
    second_rms = lax.rsqrt(jnp.sum(squares, axis=1, keepdims=True) / D + EPSILON)
    scaled = jnp.concatenate(scaled, axis=1)
    activated = []
    for n in range(4):
        for copy in up_copies[0:1] if n == 0 else up_copies[4 * n - 3 : 4 * n + 1]:
            copy.wait()
        hidden = second_rms * jnp.dot(
            scaled,
            up[:, :, 256 * n : 256 * n + 256].reshape(D, 256),
            preferred_element_type=F32,
        )
        activated.append(jnp.square(jax.nn.relu(hidden)).astype(BF16))
    activated = jnp.concatenate(activated, axis=1)
    for copy in down_copies:
        copy.wait()
    row = lax.broadcasted_iota(jnp.int32, (ROWS, 1), 0)
    mine = row // SHARE == lax.axis_index("z")
    for j in range(TP):
        part = jnp.dot(activated, down[j], preferred_element_type=F32)
        own = rows[:, :, 256 * j : 256 * j + 256].reshape(ROWS, 256).astype(F32)
        part = part + jnp.where(mine, own, 0.0)
        out[:, j] = part.astype(BF16).reshape(Z, SHARE, 256)


def mixer(rows, channel_gain, own_up, own_down, ups, downs):
    any_space = pl.BlockSpec(memory_space=pl.ANY)
    vmem = pl.BlockSpec(memory_space=pltpu.VMEM)
    return pl.pallas_call(
        mixer_kernel,
        out_shape=pltpu.VMEM((Z, TP, SHARE, 256), BF16),
        in_specs=[any_space, vmem] + [any_space] * 14,
        out_specs=vmem,
        scratch_shapes=[
            pltpu.VMEM((Z, SHARE, D), BF16),
            pltpu.VMEM((16, 128, 1024), BF16),
            pltpu.VMEM((8, 1024, 256), BF16),
            pltpu.SemaphoreType.DMA((28,)),
        ],
        compiler_params=pltpu.CompilerParams(vmem_limit_bytes=MIXER_LIMIT),
        name="mixer",
    )(
        rows, in_hbm(channel_gain.reshape(16, 128)), in_hbm(own_up.reshape(16, 128, 256)),
        in_hbm(own_down), *ups, *downs,
    )


def shift(count, by):
    return [(i, (i + by) % count) for i in range(count)]


def to_all(array, axes):
    return lax.all_to_all(array, axes, 0, 0, tiled=True)


def local(
    tokens, states, mix_gain, w_query, w_key, w_value, w_gate, head_gain, w_output,
    channel_gain, w_up, w_down,
):
    swap = [(0, 1), (1, 0)]
    blocks = [tokens] + [lax.ppermute(tokens, "y", shift(Y, by)) for by in (1, 2, 3)]
    packed_up, packed_down = pack(w_up, w_down)
    left_up = lax.ppermute(packed_up, "x", shift(X, 1))
    right_down = lax.ppermute(packed_down, "x", shift(X, 3))
    other = lax.ppermute(tokens, "c", swap)
    blocks += [other] + [lax.ppermute(block, "c", swap) for block in blocks[1:]]
    states = states.transpose(1, 2, 3, 0)
    mine, others, own, keys, values = retain(
        blocks, states, w_query, w_key, w_value, w_gate, w_output, mix_gain, head_gain
    )
    others = lax.ppermute(others, "c", swap)
    right_up = lax.ppermute(packed_up, "x", shift(X, 3))
    left_down = lax.ppermute(packed_down, "x", shift(X, 1))
    parts = pair(mine, others)
    parts = [parts[0]] + [lax.ppermute(parts[k], "y", shift(Y, k)) for k in (1, 2, 3)]
    middle = middle_rows(own, parts)
    everyone = to_all(middle, "z")
    far_up = lax.ppermute(left_up, "x", shift(X, 1))
    far_down = lax.ppermute(right_down, "x", shift(X, 3))
    near_other = [lax.ppermute(w, "c", swap) for w in (left_up, right_down)]
    near_other += [lax.ppermute(w, "c", swap) for w in (right_up, left_down)]
    keys, *near_other = lax.optimization_barrier((keys, *near_other))
    new_states = update(keys, values, states)
    far_other = [lax.ppermute(w, "c", swap) for w in (far_up, far_down)]
    near_other = [in_hbm(w) for w in near_other]
    right_up, left_down = in_hbm(right_up), in_hbm(left_down)
    far_up, far_down = in_hbm(far_up), in_hbm(far_down)
    down = mixer(
        everyone, channel_gain, w_up, w_down,
        (left_up, near_other[0], right_up, near_other[2], far_up, far_other[0]),
        (left_down, near_other[3], right_down, near_other[1], far_down, far_other[1]),
    )
    down = to_all(down.reshape(Z * TP, SHARE, 256), ("z", "y", "c"))
    layer_out = jnp.sum(down.reshape(Z, ROWS, 256).astype(F32), axis=0).astype(BF16)
    return (layer_out, new_states.transpose(3, 0, 1, 2))


def solution(mesh):
    torus = Mesh(mesh.devices.reshape(Z, X, Y, C), ("z", "x", "y", "c"))
    kv, tp = ("z", "x"), ("y", "c")
    in_specs = (
        P(kv, tp), P(kv, tp, None, None), P(), P(None, tp), P(None, tp), P(None, tp), P(None, tp),
        P(tp), P(tp, None), P(), P(None, kv), P(kv, None),
    )
    out_specs = (P(kv, tp), P(kv, tp, None, None))
    return jax.shard_map(local, mesh=torus, in_specs=in_specs, out_specs=out_specs, check_vma=False)
```
